32 devices in a mesh: grp: 2 (over y), tp: 4 (over z), dp: 4 (over x, core).
Axes of the slice: x: 2, y: 2, z: 4, core: 2. Of those that a mesh axis runs over, the one named last changes fastest.
Arguments:
- tokens: bfloat16 [128, 8, 2048], P('grp', None, 'dp'), parts along dimension 0, may hold values from -64 to 64
- live_counts: int32 [128], P(('grp', 'dp')), parts along dimension 0, may hold values from 1 to 8, 256 in all
- norm_gain: float32 [2, 2048], P(None, 'dp'), may hold values from 0.1 to 1.9
- w_branch: bfloat16 [2, 2048, 4096], P(None, 'dp', 'tp'), may hold values from -0.125 to 0.125
- w_silu_gate: bfloat16 [2, 2048, 4096], P(None, 'dp', 'tp'), may hold values from -0.125 to 0.125
- conv_weight: float32 [2, 4, 4096], P(None, None, 'tp'), may hold values from -3 to 3
- w_query: bfloat16 [2, 16, 256, 256], P(None, 'tp'), may hold values from -0.375 to 0.375
- w_key: bfloat16 [2, 16, 256, 256], P(None, 'tp'), may hold values from -0.375 to 0.375
- w_value: bfloat16 [2, 16, 256, 256], P(None, 'tp'), may hold values from -0.375 to 0.375
- w_input_gate: bfloat16 [2, 16, 768], P(None, 'tp'), may hold values from -0.21875 to 0.21875
- w_forget_gate: bfloat16 [2, 16, 768], P(None, 'tp'), may hold values from -0.21875 to 0.21875
- bias_input: float32 [2, 16], P(None, 'tp'), may hold values from -2 to 2
- bias_forget: float32 [2, 16], P(None, 'tp'), may hold values from -1 to 5
- out_gain: float32 [2, 16, 256], P(None, 'tp'), may hold values from 0.25 to 4
- skip_gain: float32 [2, 4096], P(None, 'tp'), may hold values from 0.25 to 4
- w_out: bfloat16 [2, 4096, 2048], P(None, 'tp', 'dp'), may hold values from -0.09375 to 0.09375
- conv_state: bfloat16 [2, 128, 3, 4096], P(None, ('grp', 'dp'), None, 'tp'), parts along dimension 1, may hold values from -6 to 6
- memory: float32 [2, 128, 16, 256, 256], P(None, ('grp', 'dp'), 'tp'), parts along dimension 1, may hold values from -0.375 to 0.375
- max_state: float32 [2, 128, 16], P(None, ('grp', 'dp'), 'tp'), parts along dimension 1, may hold values from -4 to 4
Outputs:
- out_tokens: bfloat16 [128, 8, 2048], P('grp', None, 'dp'), parts along dimension 0
- new_conv_state: bfloat16 [2, 128, 3, 4096], P(None, ('grp', 'dp'), None, 'tp'), parts along dimension 1
- new_memory: float32 [2, 128, 16, 256, 256], P(None, ('grp', 'dp'), 'tp'), parts along dimension 1
- new_max: float32 [2, 128, 16], P(None, ('grp', 'dp'), 'tp'), parts along dimension 1
The draws below stay inside these ranges and needn't reach their ends.
There are 2 independent parts, one for each index of `grp`. The reference program is written for one: setup_inputs(seed, part) draws one part's arguments, and reference() takes and returns one part's arrays. A program takes and returns all parts, laid end to end along the dimension named above; an argument that names none is the same for every part. Nothing has to cross between parts.
Inputs may be any that keep to these rules, and one draw needn't show every extreme that they name: `live_counts`: each sequence has at least one live slot; within each part (each independent copy of the problem) the 64 counts sum to 256, so the whole array sums to that times the number of parts; in each part some sequence uses all 8 slots.
All inputs are finite; a program needn't handle non-finite values. No bound on the sum of `live_counts` on one device may be relied on, other than what follows from the above.
Results may differ from the reference program's by a relative error of at most 0.035.
Values may be sent and summed in bfloat16 or wider, within the bound.
A program may use at most 192 MiB of HBM per device.

```python
import math
import jax
import jax.numpy as jnp
import numpy as np
from jax import lax

D = 2048
HEADS = 16
HEAD_DIM = 256
CONV = 4
LAYERS = 2
NEW = 8
BATCH = 64
INNER = 4096
N_DP = 4


def draw_tokens(key, part):
    first_key, second_key = jax.random.split(jax.random.fold_in(key, 11), 2)
    features = jnp.arange(D, dtype=jnp.float32) / D
    column_scale = jnp.exp(jnp.log(6.0) * features + jax.random.uniform(second_key, (D,), jnp.float32, -0.4, 0.4))
    base = jnp.clip(jax.random.normal(first_key, (BATCH, NEW, D), jnp.float32), -4.0, 4.0)
    return (base * column_scale).astype(jnp.bfloat16)


def block_scale(own_key, dims, pieces, low, largest):
    level, own = 1.0, jax.random.fold_in(own_key, 6)
    for position, shards_of in pieces:
        steps = jnp.exp(jax.random.uniform(jax.random.fold_in(own, position), (shards_of,), jnp.float32, low / len(pieces), largest / len(pieces)))
        level = level * jnp.repeat(steps, dims[position] // shards_of).reshape([-1 if axis == position else 1 for axis in range(len(dims))])
    return level


def length_profile(count, total, bound, lean):
    weights = [(1 << 20) // math.isqrt(standing ** lean) + 1 for standing in range(2, count + 1)]
    surplus, holding = total - bound - (count - 1), [1] * (count - 1)
    while surplus > 0:
        movable = [i for i in range(count - 1) if holding[i] < bound]
        pool, budget = sum([weights[i] for i in movable]), surplus
        for i in movable:
            extra = min(bound - holding[i], max(1, budget * weights[i] // pool), surplus)
            holding[i] = holding[i] + extra
            surplus = surplus - extra
    return np.array([bound] + holding)


def uneven(key, number_of, total, bound, slope):
    if number_of == 2:
        one = jax.random.randint(key, (), max(1, total - bound), min(bound, total - 1) + 1)
        return jnp.stack([one, total - one])
    tallies = jnp.asarray(length_profile(number_of, total, bound, slope), jnp.int32)
    pairs = (number_of - 1) // 2
    donor, receiver = tallies[1:1 + 2 * pairs:2], tallies[2:2 + 2 * pairs:2]
    margin = jnp.minimum(donor - 1, bound - receiver)
    shifted = jax.random.randint(jax.random.fold_in(key, 1), (pairs,), 0, 1 << 20) % (margin + 1)
    tallies = tallies.at[1:1 + 2 * pairs:2].set(donor - shifted).at[2:2 + 2 * pairs:2].set(receiver + shifted)
    return tallies[jax.random.permutation(jax.random.fold_in(key, 2), number_of)]


def normal_values(rng, dims, deviation, most, cuts=(), kind=jnp.bfloat16):
    level = block_scale(rng, dims, cuts, -0.22, 0.18) if cuts else 1.0
    entries = jax.random.normal(rng, dims, jnp.float32) * deviation * level
    return jnp.minimum(jnp.maximum(entries, -most), most).astype(kind)


def setup_inputs(seed: int = 0, part: int = 0) -> dict:
    keys = jax.random.split(jax.random.key(seed), 20)
    part_keys = jax.random.split(jax.random.fold_in(keys[19], part), 20)
    return {
        "tokens": draw_tokens(jax.random.fold_in(jax.random.fold_in(keys[19], part), 71), part),
        "live_counts": uneven(part_keys[1], BATCH, BATCH * NEW // 2, NEW, 2).astype(jnp.int32),
        "norm_gain": jnp.clip(1.0 + 0.18 * jax.random.normal(keys[2], (LAYERS, D), jnp.float32), 0.1, 1.9),
        "w_branch": normal_values(keys[3], (LAYERS, D, INNER), D ** -0.5, 0.125, ((1, 4), (2, 4))),
        "w_silu_gate": normal_values(keys[4], (LAYERS, D, INNER), D ** -0.5, 0.125, ((1, 4), (2, 4))),
        "conv_weight": normal_values(keys[5], (LAYERS, CONV, INNER), CONV ** -0.5, 3.0, ((2, 4),), jnp.float32),
        "w_query": normal_values(keys[6], (LAYERS, HEADS, HEAD_DIM, HEAD_DIM), HEAD_DIM ** -0.5, 0.375, ((1, 4),)),
        "w_key": normal_values(keys[7], (LAYERS, HEADS, HEAD_DIM, HEAD_DIM), HEAD_DIM ** -0.5, 0.375, ((1, 4),)),
        "w_value": normal_values(keys[8], (LAYERS, HEADS, HEAD_DIM, HEAD_DIM), HEAD_DIM ** -0.5, 0.375, ((1, 4),)),
        "w_input_gate": normal_values(keys[9], (LAYERS, HEADS, 3 * HEAD_DIM), (3 * HEAD_DIM) ** -0.5, 0.21875, ((1, 4),)),
        "w_forget_gate": normal_values(keys[10], (LAYERS, HEADS, 3 * HEAD_DIM), (3 * HEAD_DIM) ** -0.5, 0.21875, ((1, 4),)),
        "bias_input": jnp.clip(jax.random.uniform(keys[11], (LAYERS, HEADS), jnp.float32, -2.0, 2.0) * block_scale(keys[11], (LAYERS, HEADS), ((1, 4),), -0.4, 0.0), -2.0, 2.0),
        "bias_forget": jnp.clip(-1.0 + 6.0 * jax.random.uniform(keys[12], (LAYERS, HEADS), jnp.float32) ** block_scale(keys[12], (LAYERS, HEADS), ((1, 4),), -0.2, 0.2), -1.0, 5.0),
        "out_gain": jnp.clip(jnp.exp(math.log(4.0) - 2.7725887 * jax.random.uniform(keys[13], (LAYERS, HEADS, HEAD_DIM), jnp.float32) ** block_scale(keys[13], (LAYERS, HEADS, HEAD_DIM), ((1, 4),), -0.2, 0.2)), 0.25, 4.0),
        "skip_gain": jnp.clip(jnp.exp(math.log(4.0) - 2.7725887 * jax.random.uniform(keys[14], (LAYERS, INNER), jnp.float32) ** block_scale(keys[14], (LAYERS, INNER), ((1, 4),), -0.2, 0.2)), 0.25, 4.0),
        "w_out": normal_values(keys[15], (LAYERS, INNER, D), INNER ** -0.5, 0.09375, ((1, 4), (2, 4))),
        "conv_state": normal_values(part_keys[16], (LAYERS, BATCH, CONV - 1, INNER), 1.0, 6.0, ((1, 4), (3, 4))),
        "memory": normal_values(part_keys[17], (LAYERS, BATCH, HEADS, HEAD_DIM, HEAD_DIM), (HEAD_DIM ** -0.5), 0.375, ((1, 4), (2, 4)), jnp.float32),
        "max_state": normal_values(part_keys[18], (LAYERS, BATCH, HEADS), 1.0, 4.0, ((1, 4), (2, 4)), jnp.float32),
    }


epsilon = 1e-06
very_negative = -1e+30

def layer_step(tokens, live_counts, gain, w_branch, w_silu_gate, conv_weight, w_query, w_key, w_value, w_input_gate, w_forget_gate, bias_input, bias_forget, out_gain, skip_gain, w_out, conv_state, memory, max_state):
    floats = tokens.astype(jnp.float32)
    mean_square = lax.optimization_barrier(jnp.mean(floats * floats, axis=-1, keepdims=True))
    normed = (floats * lax.rsqrt(mean_square + epsilon) * gain).astype(jnp.bfloat16)
    flat = normed.reshape(BATCH * NEW, D)
    block_rows = D // N_DP
    branch_sum = jnp.zeros((BATCH * NEW, INNER), jnp.float32)
    gate_sum = jnp.zeros((BATCH * NEW, INNER), jnp.float32)
    for block in range(N_DP):
        lower = block * block_rows
        rows = flat[:, lower:lower + block_rows]
        first = jnp.dot(rows, w_branch[lower:lower + block_rows], preferred_element_type=jnp.float32)
        second = jnp.dot(rows, w_silu_gate[lower:lower + block_rows], preferred_element_type=jnp.float32)
        branch_sum = branch_sum + first.astype(jnp.bfloat16).astype(jnp.float32)
        gate_sum = gate_sum + second.astype(jnp.bfloat16).astype(jnp.float32)
    branch = branch_sum.astype(jnp.bfloat16).reshape(BATCH, NEW, INNER)
    silu_gate = gate_sum.astype(jnp.bfloat16).reshape(BATCH, NEW, INNER)
    padded = jnp.concatenate([conv_state, branch], axis=1)
    conv_sum = jnp.zeros((BATCH, NEW, INNER), jnp.float32)
    for offset in range(CONV):
        conv_sum = conv_sum + padded[:, offset:offset + NEW].astype(jnp.float32) * conv_weight[offset]
    convolved = jax.nn.silu(conv_sum).astype(jnp.bfloat16)
    picks = live_counts[:, None] + jnp.arange(CONV - 1, dtype=jnp.int32)[None, :]
    new_conv = jnp.take_along_axis(padded, picks[:, :, None], axis=1)
    conv_heads = convolved.reshape(BATCH, NEW, HEADS, HEAD_DIM).astype(jnp.float32)
    branch_heads = branch.reshape(BATCH, NEW, HEADS, HEAD_DIM).astype(jnp.float32)
    queries = jnp.einsum('blhd,hde->blhe', conv_heads, w_query.astype(jnp.float32)).astype(jnp.bfloat16)
    key_rows = jnp.einsum('blhd,hde->blhe', conv_heads, w_key.astype(jnp.float32)).astype(jnp.bfloat16)
    value_rows = jnp.einsum('blhd,hde->blhe', branch_heads, w_value.astype(jnp.float32)).astype(jnp.bfloat16)
    joined = jnp.concatenate([queries, key_rows, value_rows], axis=-1).astype(jnp.float32)
    input_log = jnp.einsum('blhc,hc->blh', joined, w_input_gate.astype(jnp.float32)) + bias_input
    forget_log = jax.nn.log_sigmoid(jnp.einsum('blhc,hc->blh', joined, w_forget_gate.astype(jnp.float32)) + bias_forget)
    positions = jnp.arange(NEW, dtype=jnp.int32)
    live = positions[None, :] < live_counts[:, None]
    input_log = jnp.transpose(jnp.where(live[:, :, None], input_log, very_negative), (0, 2, 1))
    forget_log = jnp.transpose(jnp.where(live[:, :, None], forget_log, 0.0), (0, 2, 1))
    query_heads = jnp.transpose(queries.astype(jnp.float32), (0, 2, 1, 3))
    key_heads = jnp.transpose(key_rows.astype(jnp.float32), (0, 2, 1, 3)) * HEAD_DIM ** (-0.5)
    value_heads = jnp.transpose(value_rows.astype(jnp.float32), (0, 2, 1, 3))
    cumulative = jnp.cumsum(forget_log, axis=-1)
    log_weights = cumulative[..., :, None] - cumulative[..., None, :] + input_log[..., None, :]
    causal = positions[:, None] >= positions[None, :]
    log_weights = jnp.where(causal, log_weights, very_negative)
    carried = cumulative + max_state[..., None]
    stabilizer = jnp.maximum(lax.optimization_barrier(jnp.max(log_weights, axis=-1)), carried)
    weights = jnp.exp(log_weights - stabilizer[..., None])
    carried_scale = jnp.exp(carried - stabilizer)
    scores = jnp.einsum('bhtd,bhsd->bhts', query_heads, key_heads) * weights
    numerator = jnp.einsum('bhts,bhse->bhte', scores, value_heads)
    numerator = numerator + carried_scale[..., None] * jnp.einsum('bhtd,bhde->bhte', query_heads, memory)
    centered = numerator - lax.optimization_barrier(jnp.mean(numerator, axis=-1, keepdims=True))
    normalized = centered * lax.rsqrt(lax.optimization_barrier(jnp.mean(centered * centered, axis=-1, keepdims=True)) + epsilon)
    normalized = normalized * out_gain[None, :, None, :]
    readout = jnp.transpose(normalized, (0, 2, 1, 3)).reshape(BATCH, NEW, INNER)
    new_max = stabilizer[..., -1]
    decay = jnp.exp(cumulative[..., -1] + max_state - new_max)
    update_weight = jnp.exp(cumulative[..., -1:] - cumulative + input_log - new_max[..., None])
    new_memory = decay[..., None, None] * memory + jnp.einsum('bhs,bhsd,bhse->bhde', update_weight, key_heads, value_heads)
    mixed = (readout + skip_gain * convolved.astype(jnp.float32)) * jax.nn.silu(silu_gate.astype(jnp.float32))
    mixed = jnp.where(live[:, :, None], mixed, 0.0).astype(jnp.bfloat16)
    projected = jnp.dot(mixed.reshape(BATCH * NEW, INNER), w_out, preferred_element_type=jnp.float32)
    projected = projected.astype(jnp.bfloat16).reshape(BATCH, NEW, D)
    result = (floats + projected.astype(jnp.float32)).astype(jnp.bfloat16)
    return (result, new_conv, new_memory, new_max)

def reference(tokens, live_counts, norm_gain, w_branch, w_silu_gate, conv_weight, w_query, w_key, w_value, w_input_gate, w_forget_gate, bias_input, bias_forget, out_gain, skip_gain, w_out, conv_state, memory, max_state):
    stream = tokens
    conv_list = []
    memory_list = []
    max_list = []
    for which_layer in range(LAYERS):
        stream, new_conv, new_memory, new_max = layer_step(stream, live_counts, norm_gain[which_layer], w_branch[which_layer], w_silu_gate[which_layer], conv_weight[which_layer], w_query[which_layer], w_key[which_layer], w_value[which_layer], w_input_gate[which_layer], w_forget_gate[which_layer], bias_input[which_layer], bias_forget[which_layer], out_gain[which_layer], skip_gain[which_layer], w_out[which_layer], conv_state[which_layer], memory[which_layer], max_state[which_layer])
        conv_list.append(new_conv)
        memory_list.append(new_memory)
        max_list.append(new_max)
    return (stream, jnp.stack(conv_list), jnp.stack(memory_list), jnp.stack(max_list))
```

```python
import functools

import jax
import jax.numpy as jnp
from jax import lax
from jax.experimental import pallas as pl
from jax.experimental.pallas import tpu as pltpu
from jax.sharding import PartitionSpec as P

HEAD_DIM = 256
CONV = 4
LAYERS = 2
epsilon = 1e-06
very_negative = -1e30

VM = pl.BlockSpec(memory_space=pltpu.VMEM)
MESH = pl.DeviceIdType.MESH


def greet(axis, devices):
    barrier = pltpu.get_barrier_semaphore()
    for device in devices:
        pl.semaphore_signal(barrier, inc=1, device_id={axis: device}, device_id_type=MESH)
    pl.semaphore_wait(barrier, len(devices))


def rcopy(src, dst, send, recv, axis, device):
    return pltpu.make_async_remote_copy(
        src_ref=src, dst_ref=dst, send_sem=send, recv_sem=recv,
        device_id={axis: device}, device_id_type=MESH,
    )


def scatter_kernel(n, chunks, a_ref, b_ref, aux_ref, oa_ref, ob_ref, oaux_ref,
                   r1a, r1b, s2a, s2b, r2a, r2b, s1s, s1r, s2s, s2r, axs, axr):
    nx = n // 2
    me = lax.axis_index("dp")
    core = me % 2
    x = me // 2
    partner = me + 1 - 2 * core
    greet("dp", [(me + off) % n for off in range(1, n)])
    started = []
    aux_copies = []
    first = {}
    for g in range(nx):
        xo = (x + 1 + g) % nx
        for c in range(chunks):
            pair = []
            for k, (src, dst) in enumerate(((a_ref, r1a), (b_ref, r1b))):
                cp = rcopy(src.at[xo, 1 - core, c], dst.at[g, c],
                           s1s.at[g, c, k], s1r.at[g, c, k], "dp", partner)
                cp.start()
                pair.append(cp)
                started.append(cp)
            first[g, c] = pair
        if g == 0:
            for off in range(1, n):
                to = (me + off) % n
                cp = rcopy(aux_ref.at[to], oaux_ref.at[me], axs.at[off - 1], axr.at[off - 1], "dp", to)
                cp.start()
                aux_copies.append(cp)
                started.append(cp)
            oaux_ref[me] = aux_ref[me]
    second = {}
    for g in range(nx - 1):
        xo = (x + 1 + g) % nx
        for c in range(chunks):
            pair = []
            for k, (src, got, buf, dst) in enumerate(((a_ref, r1a, s2a, r2a), (b_ref, r1b, s2b, r2b))):
                first[g, c][k].wait_recv()
                buf[g, c] = (
                    src[xo, core, c].astype(jnp.float32) + got[g, c].astype(jnp.float32)
                ).astype(jnp.bfloat16)
                cp = rcopy(buf.at[g, c], dst.at[g, c], s2s.at[g, c, k], s2r.at[g, c, k],
                           "dp", 2 * xo + core)
                cp.start()
                pair.append(cp)
                started.append(cp)
            second[g, c] = pair
    for c in range(chunks):
        for k, (src, got, more, out) in enumerate(((a_ref, r1a, r2a, oa_ref), (b_ref, r1b, r2b, ob_ref))):
            first[nx - 1, c][k].wait_recv()
            total = src[x, core, c].astype(jnp.float32) + got[nx - 1, c].astype(jnp.float32)
            for g in range(nx - 1):
                second[g, c][k].wait_recv()
                total = total + more[g, c].astype(jnp.float32)
            out[c] = total
    for cp in aux_copies:
        cp.wait_recv()
    for cp in started:
        cp.wait_send()


def scatter_dp(n, a, b, aux):
    rows, width = a.shape
    nx = n // 2
    own = rows // n
    chunks = 4 if own % 64 == 0 else 1
    piece = own // chunks
    a = a.reshape(nx, 2, chunks, piece, width)
    b = b.reshape(nx, 2, chunks, piece, width)
    far = max(nx - 1, 1)
    bf = jnp.bfloat16
    sem = pltpu.SemaphoreType.DMA
    oa, ob, oaux = pl.pallas_call(
        functools.partial(scatter_kernel, n, chunks),
        out_shape=(
            jax.ShapeDtypeStruct((chunks, piece, width), jnp.float32),
            jax.ShapeDtypeStruct((chunks, piece, width), jnp.float32),
            jax.ShapeDtypeStruct(aux.shape, jnp.float32),
        ),
        in_specs=[VM] * 3,
        out_specs=(VM,) * 3,
        scratch_shapes=[
            pltpu.VMEM((nx, chunks, piece, width), bf),
            pltpu.VMEM((nx, chunks, piece, width), bf),
            pltpu.VMEM((far, chunks, piece, width), bf),
            pltpu.VMEM((far, chunks, piece, width), bf),
            pltpu.VMEM((far, chunks, piece, width), bf),
            pltpu.VMEM((far, chunks, piece, width), bf),
            sem((nx, chunks, 2)), sem((nx, chunks, 2)),
            sem((far, chunks, 2)), sem((far, chunks, 2)),
            sem((n - 1,)), sem((n - 1,)),
        ],
        compiler_params=pltpu.CompilerParams(collective_id=0, has_side_effects=True),
        name="scatter_dp",
    )(a, b, aux)
    return oa.reshape(own, width), ob.reshape(own, width), oaux


def gather_kernel(n, chunks, m_ref, out_ref, xs, xr, ps, pr, fs, fr):
    nx = n // 2
    me = lax.axis_index("dp")
    core = me % 2
    x = me // 2
    partner = me + 1 - 2 * core
    greet("dp", [partner] + [2 * ((x + 1 + g) % nx) + core for g in range(nx - 1)])
    started = []
    across = {}
    near = {}
    for c in range(chunks):
        for g in range(nx - 1):
            to = 2 * ((x + 1 + g) % nx) + core
            cp = rcopy(m_ref.at[c], out_ref.at[x, core, c], xs.at[g, c], xr.at[g, c], "dp", to)
            cp.start()
            across[g, c] = cp
            started.append(cp)
    for c in range(chunks):
        cp = rcopy(m_ref.at[c], out_ref.at[x, core, c], ps.at[c], pr.at[c], "dp", partner)
        cp.start()
        near[c] = cp
        started.append(cp)
    out_ref[x, core] = m_ref[...]
    passed = []
    for c in range(chunks):
        for g in range(nx - 1):
            origin = (x + nx - 1 - g) % nx
            across[g, c].wait_recv()
            cp = rcopy(out_ref.at[origin, core, c], out_ref.at[origin, core, c],
                       fs.at[g, c], fr.at[g, c], "dp", partner)
            cp.start()
            passed.append(cp)
            started.append(cp)
    for c in range(chunks):
        near[c].wait_recv()
    for cp in passed:
        cp.wait_recv()
    for cp in started:
        cp.wait_send()


def gather_dp(n, m):
    own, width = m.shape
    nx = n // 2
    chunks = 4 if own % 64 == 0 else 1
    piece = own // chunks
    far = max(nx - 1, 1)
    sem = pltpu.SemaphoreType.DMA
    out = pl.pallas_call(
        functools.partial(gather_kernel, n, chunks),
        out_shape=jax.ShapeDtypeStruct((nx, 2, chunks, piece, width), m.dtype),
        in_specs=[VM],
        out_specs=VM,
        scratch_shapes=[
            sem((far, chunks)), sem((far, chunks)), sem((chunks,)), sem((chunks,)),
            sem((far, chunks)), sem((far, chunks)),
        ],
        compiler_params=pltpu.CompilerParams(collective_id=1, has_side_effects=True),
        name="gather_dp",
    )(m.reshape(chunks, piece, width))
    return out.reshape(n * own, width)


def reduce_kernel(n, p_ref, x_ref, out_ref, got, mine, s1, r1, s2, r2):
    me = lax.axis_index("tp")
    greet("tp", [(me + off) % n for off in range(1, n)])
    started = []
    first = []
    order = sorted(range(1, n), key=lambda off: -min(off, n - off))
    for off in order:
        to = (me + off) % n
        cp = rcopy(p_ref.at[to], got.at[off - 1], s1.at[off - 1], r1.at[off - 1], "tp", to)
        cp.start()
        started.append(cp)
        first.append((off, cp))
    total = p_ref[me].astype(jnp.float32)
    for off, cp in first:
        cp.wait_recv()
        total = total + got[off - 1].astype(jnp.float32)
    update = total.astype(jnp.bfloat16).astype(jnp.float32)
    mine[...] = (x_ref[me].astype(jnp.float32) + update).astype(jnp.bfloat16)
    second = []
    for off in order:
        to = (me + off) % n
        cp = rcopy(mine, out_ref.at[me], s2.at[off - 1], r2.at[off - 1], "tp", to)
        cp.start()
        started.append(cp)
        second.append(cp)
    out_ref[me] = mine[...]
    for cp in second:
        cp.wait_recv()
    for cp in started:
        cp.wait_send()


def reduce_tp(n, p, x):
    rows, width = p.shape
    share = rows // n
    sem = pltpu.SemaphoreType.DMA
    out = pl.pallas_call(
        functools.partial(reduce_kernel, n),
        out_shape=jax.ShapeDtypeStruct((n, share, width), jnp.bfloat16),
        in_specs=[VM] * 2,
        out_specs=VM,
        scratch_shapes=[
            pltpu.VMEM((n - 1, share, width), jnp.bfloat16),
            pltpu.VMEM((share, width), jnp.bfloat16),
            sem((n - 1,)), sem((n - 1,)), sem((n - 1,)), sem((n - 1,)),
        ],
        compiler_params=pltpu.CompilerParams(collective_id=2, has_side_effects=True),
        name="reduce_tp",
    )(p.reshape(n, share, width), x.reshape(n, share, width))
    return out.reshape(rows, width)


def cell_kernel(layer, model, heads, steps, cnt_ref, bi_ref, bf_ref, br_ref, gt_ref, aux_ref,
                ccol_ref, crow_ref, mcol_ref, st_ref, cw_ref, wq_ref, wk_ref, wv_ref, wg_ref,
                og_ref, sg_ref, mem_ref, *rest):
    (mixed_ref, nc_ref, newmem_ref, nmax_ref,
     pad_s, conv_s, q_s, k_s, v_s, num_s, car_s, dec_s, cs_s, top_s, nc_s, stage, ins, outs) = rest[-18:]
    f32 = jnp.float32
    bf = jnp.bfloat16
    batch = stage.shape[0]
    own, width = br_ref.shape
    dim = HEAD_DIM
    base = 8 - (CONV - 1)

    def fetch(b):
        return pltpu.make_async_copy(mem_ref.at[layer, b], stage.at[b], ins.at[b])

    def store(b):
        return pltpu.make_async_copy(stage.at[b], newmem_ref.at[layer, b], outs.at[b])

    for b in range(batch):
        fetch(b).start()

    squares = aux_ref[0, 0:1, :own]
    for i in range(1, aux_ref.shape[0]):
        squares = squares + aux_ref[i, 0:1, :own]
    inv_row = lax.rsqrt(squares / model + epsilon)
    r = lax.broadcasted_iota(jnp.int32, (own, own), 0)
    c = lax.broadcasted_iota(jnp.int32, (own, own), 1)
    inv = jnp.sum(jnp.where(r == c, inv_row, 0.0), axis=1, keepdims=True)
    branch = (br_ref[...] * inv).astype(bf)
    pad_s[:, 8:8 + steps, :] = branch.astype(f32).reshape(batch, steps, width)
    for j in range(CONV - 1):
        rows = st_ref[0, j].astype(f32)
        for b in range(batch):
            pad_s[b, base + j:base + j + 1, :] = rows[b:b + 1, :]
    total = pad_s[:, base:base + steps, :] * cw_ref[0, 0:1, :]
    for j in range(1, CONV):
        total = total + pad_s[:, base + j:base + j + steps, :] * cw_ref[0, j:j + 1, :]
    conv = (total * jax.nn.sigmoid(total)).astype(bf).reshape(own, width)
    conv_s[...] = conv
    for b in range(batch):
        for i in range(CONV - 1):
            nc_s[i, b:b + 1, :] = pad_s[b, pl.ds(base + i + cnt_ref[b], 1), :]
    nc_ref[...] = nc_s[...].astype(bf)

    same = (r // steps) == (c // steps)
    causal = same & (r >= c)
    behind = same & (r <= c)
    live_col = (r[:, 0:1] % steps) < ccol_ref[...]
    live_row = (c[0:1, :] % steps) < crow_ref[...]
    nt = (((1,), (1,)), ((), ()))
    for h in range(heads):
        sl = slice(h * dim, (h + 1) * dim)
        q = jnp.dot(conv[:, sl], wq_ref[0, h], preferred_element_type=f32).astype(bf)
        k = jnp.dot(conv[:, sl], wk_ref[0, h], preferred_element_type=f32).astype(bf)
        v = jnp.dot(branch[:, sl], wv_ref[0, h], preferred_element_type=f32).astype(bf)
        gcol = None
        for i, part in enumerate((q, k, v)):
            w = wg_ref[0, h, :, i * dim:(i + 1) * dim]
            one = lax.dot_general(part, w, nt, preferred_element_type=f32)
            two = lax.dot_general(w, part, nt, preferred_element_type=f32)
            gcol, grow = (one, two) if gcol is None else (gcol + one, grow + two)
        bias_i = bi_ref[layer, h]
        bias_f = bf_ref[layer, h]

        def log_sig(x):
            return jnp.minimum(x, 0.0) - jnp.log1p(jnp.exp(-jnp.abs(x)))

        ig_col = jnp.where(live_col, gcol[:, 0:1] + bias_i, very_negative)
        ig_row = jnp.where(live_row, grow[0:1, :] + bias_i, very_negative)
        fg_col = jnp.where(live_col, log_sig(gcol[:, 1:2] + bias_f), 0.0)
        fg_row = jnp.where(live_row, log_sig(grow[1:2, :] + bias_f), 0.0)
        cum_col = jnp.sum(jnp.where(causal, fg_row, 0.0), axis=1, keepdims=True)
        end_col = jnp.sum(jnp.where(same, fg_row, 0.0), axis=1, keepdims=True)
        cum_row = jnp.sum(jnp.where(behind, fg_col, 0.0), axis=0, keepdims=True)
        lift_row = ig_row - cum_row
        logw = jnp.where(causal, cum_col + lift_row, very_negative)
        old_max = mcol_ref[:, h:h + 1]
        carried = cum_col + old_max
        stab = jnp.maximum(jnp.max(logw, axis=1, keepdims=True), carried)
        weights = jnp.exp(logw - stab)
        top = jnp.max(jnp.where(same, end_col + lift_row, very_negative), axis=1, keepdims=True)
        new_max = jnp.maximum(top, end_col + old_max)
        update = jnp.exp(end_col - cum_col + ig_col - new_max)
        top_s[:, h:h + 1] = new_max
        dec_s[:, h:h + 1] = jnp.exp(end_col + old_max - new_max)
        cs_s[:, h:h + 1] = jnp.exp(carried - stab)
        scores = lax.dot_general(q, k, nt, preferred_element_type=f32)
        scores = (jnp.where(causal, scores, 0.0) * (dim ** -0.5) * weights).astype(bf)
        num_s[:, sl] = jnp.dot(scores, v, preferred_element_type=f32)
        q_s[:, sl] = q.astype(f32)
        k_s[:, sl] = k.astype(f32) * (dim ** -0.5) * update
        v_s[:, sl] = v.astype(f32)
    nmax_ref[...] = top_s[pl.ds(steps - 1, batch, stride=steps), :]

    @pl.loop(0, batch)
    def _(b):
        fetch(b).wait()
        rows = pl.ds(pl.multiple_of(b * steps, 8), steps)
        for h in range(heads):
            sl = slice(h * dim, (h + 1) * dim)
            old = stage[b, h]
            car_s[rows, sl] = jnp.dot(q_s[rows, sl].astype(bf), old.astype(bf), preferred_element_type=f32)
            outer = lax.dot_general(
                k_s[rows, sl].astype(bf), v_s[rows, sl].astype(bf), (((0,), (0,)), ((), ())),
                preferred_element_type=f32,
            )
            stage[b, h] = dec_s[rows, :][0:1, h:h + 1] * old + outer
        store(b).start()

    live = (lax.broadcasted_iota(jnp.int32, (own, 1), 0) % steps) < ccol_ref[...]
    for h in range(heads):
        sl = slice(h * dim, (h + 1) * dim)
        num = num_s[:, sl] + cs_s[:, h:h + 1] * car_s[:, sl]
        centered = num - jnp.mean(num, axis=1, keepdims=True)
        normal = centered * lax.rsqrt(jnp.mean(centered * centered, axis=1, keepdims=True) + epsilon)
        gate = (gt_ref[:, sl] * inv).astype(bf).astype(f32)
        mixed = normal * og_ref[0, h:h + 1, :] + sg_ref[layer:layer + 1, sl] * conv_s[:, sl].astype(f32)
        mixed = mixed * (gate * jax.nn.sigmoid(gate))
        mixed_ref[:, sl] = jnp.where(live, mixed, 0.0).astype(bf)
    for b in range(batch):
        store(b).wait()


def memory_cell(layer, model, steps, counts, bias_input, bias_forget, branch, gate, aux, count_col,
                count_row, old_max, state, conv_weight, w_query, w_key, w_value, w_gates, out_gain,
                skip_gain, memory, previous):
    _, batch, heads, dim, _ = memory.shape
    own, width = branch.shape
    f32 = jnp.float32

    def whole(a):
        return pl.BlockSpec(a.shape, lambda i: (0,) * a.ndim)

    def layered(a):
        return pl.BlockSpec((1,) + a.shape[1:], lambda i: (layer,) + (0,) * (a.ndim - 1))

    smem = pl.BlockSpec(memory_space=pltpu.SMEM)
    anyspace = pl.BlockSpec(memory_space=pl.ANY)
    args = [counts, bias_input, bias_forget, branch, gate, aux, count_col, count_row, old_max,
            state, conv_weight, w_query, w_key, w_value, w_gates, out_gain, skip_gain, memory]
    specs = [smem, smem, smem] + [whole(a) for a in args[3:9]] + [layered(a) for a in args[9:16]]
    specs += [whole(skip_gain), anyspace]
    aliases = {}
    if previous is not None:
        aliases = {len(args): 2}
        args.append(previous)
        specs.append(anyspace)
    big = pltpu.VMEM((own, width), f32)
    small = pltpu.VMEM((own, 128), f32)
    return pl.pallas_call(
        functools.partial(cell_kernel, layer, model, heads, steps),
        grid=(1,),
        out_shape=(
            jax.ShapeDtypeStruct((own, width), jnp.bfloat16),
            jax.ShapeDtypeStruct((CONV - 1, batch, width), jnp.bfloat16),
            jax.ShapeDtypeStruct(memory.shape, f32),
            jax.ShapeDtypeStruct((batch, 128), f32),
        ),
        in_specs=specs,
        out_specs=(
            pl.BlockSpec((own, width), lambda i: (0, 0)),
            pl.BlockSpec((CONV - 1, batch, width), lambda i: (0, 0, 0)),
            anyspace,
            pl.BlockSpec((batch, 128), lambda i: (0, 0)),
        ),
        scratch_shapes=[
            pltpu.VMEM((batch, 8 + steps, width), f32),
            pltpu.VMEM((own, width), jnp.bfloat16),
            big, big, big, big, big, small, small, small,
            pltpu.VMEM((CONV - 1, batch, width), f32),
            pltpu.VMEM((batch, heads, dim, dim), f32),
            pltpu.SemaphoreType.DMA((batch,)), pltpu.SemaphoreType.DMA((batch,)),
        ],
        input_output_aliases=aliases,
        compiler_params=pltpu.CompilerParams(dimension_semantics=("arbitrary",)),
        name="memory_cell",
    )(*args)


def per_device(tokens, live_counts, norm_gain, w_branch, w_silu_gate, conv_weight, w_query, w_key,
               w_value, w_input_gate, w_forget_gate, bias_input, bias_forget, out_gain, skip_gain,
               w_out, conv_state, memory, max_state):
    f32 = jnp.float32
    bf = jnp.bfloat16
    ndp = lax.axis_size("dp")
    ntp = lax.axis_size("tp")
    all_batch, steps, features = tokens.shape
    batch = live_counts.shape[0]
    width = w_branch.shape[2]
    heads = w_query.shape[1]
    rows = all_batch * steps
    own = batch * steps
    live_rows = all_batch * steps // 2
    lanes = -(-own // 128) * 128
    model = features * ndp
    flat_tokens = tokens.reshape(rows, features)
    positions = jnp.arange(steps, dtype=jnp.int32)
    count_row = jnp.pad(live_counts.astype(f32), (0, lanes - batch))

    count_col = jnp.repeat(live_counts, steps)[:, None]
    count_lane = jnp.repeat(live_counts, steps)[None, :]
    old_max = jnp.repeat(max_state, steps, axis=1)
    states = jnp.transpose(conv_state, (0, 2, 1, 3))
    w_gates = jnp.pad(jnp.stack([w_input_gate, w_forget_gate], axis=2), ((0, 0), (0, 0), (0, 6), (0, 0)))

    dense = flat_tokens
    compact = None
    select = None
    live_all = None
    new_memory = None
    conv_list = []
    max_list = []
    for l in range(LAYERS):
        floats = dense.astype(f32)
        squares = jnp.sum(floats * floats, axis=-1).reshape(ndp, own)
        squares = jnp.pad(squares, ((0, 0), (0, lanes - own)))
        aux = jnp.stack([squares, jnp.broadcast_to(count_row, squares.shape)], axis=1)
        aux = jnp.pad(aux, ((0, 0), (0, 6), (0, 0)))
        scaled = (floats * norm_gain[l]).astype(bf)
        first = jnp.dot(scaled, w_branch[l], preferred_element_type=f32).astype(bf)
        second = jnp.dot(scaled, w_silu_gate[l], preferred_element_type=f32).astype(bf)
        branch, gate, aux = scatter_dp(ndp, first, second, aux)
        if select is None:
            counts = aux[:, 1, :batch].astype(jnp.int32).reshape(all_batch)
            ids = jnp.arange(all_batch)
            before = jnp.sum(jnp.where(ids[None, :] < ids[:, None], counts[None, :], 0), axis=1)
            live_all = positions[None, :] < counts[:, None]
            place = jnp.where(live_all, before[:, None] + positions[None, :], -1).reshape(rows)
            select = (jnp.arange(live_rows)[:, None] == place[None, :]).astype(bf)
            compact = jnp.dot(select, flat_tokens, preferred_element_type=f32).astype(bf)

        mixed, new_conv, new_memory, new_max = memory_cell(
            l, model, steps, live_counts, bias_input, bias_forget, branch, gate, aux, count_col,
            count_lane, old_max[l], states, conv_weight, w_query, w_key, w_value, w_gates,
            out_gain, skip_gain, memory, new_memory
        )
        conv_list.append(new_conv)
        max_list.append(new_max[:, :heads])
        everyone = gather_dp(ndp, mixed)
        packed = jnp.dot(select, everyone, preferred_element_type=f32).astype(bf)
        part = jnp.dot(packed, w_out[l], preferred_element_type=f32).astype(bf)
        compact = reduce_tp(ntp, part, compact)
        dense = lax.dot_general(
            select, compact, (((0,), (0,)), ((), ())), preferred_element_type=f32
        ).astype(bf)
    result = jnp.where(live_all[:, :, None], dense.reshape(tokens.shape), tokens)
    return (result, jnp.transpose(jnp.stack(conv_list), (0, 2, 1, 3)), new_memory, jnp.stack(max_list))


def solution(mesh):
    in_specs = (
        P("grp", None, "dp"),
        P(("grp", "dp")),
        P(None, "dp"),
        P(None, "dp", "tp"),
        P(None, "dp", "tp"),
        P(None, None, "tp"),
        P(None, "tp", None, None),
        P(None, "tp", None, None),
        P(None, "tp", None, None),
        P(None, "tp", None),
        P(None, "tp", None),
        P(None, "tp"),
        P(None, "tp"),
        P(None, "tp", None),
        P(None, "tp"),
        P(None, "tp", "dp"),
        P(None, ("grp", "dp"), None, "tp"),
        P(None, ("grp", "dp"), "tp", None, None),
        P(None, ("grp", "dp"), "tp"),
    )
    out_specs = (
        P("grp", None, "dp"),
        P(None, ("grp", "dp"), None, "tp"),
        P(None, ("grp", "dp"), "tp", None, None),
        P(None, ("grp", "dp"), "tp"),
    )
    return jax.shard_map(
        per_device, mesh=mesh, in_specs=in_specs, out_specs=out_specs, check_vma=False
    )
```

```python
import functools

import jax
import jax.numpy as jnp
from jax import lax
from jax.experimental import pallas as pl
from jax.experimental.pallas import tpu as pltpu
from jax.sharding import PartitionSpec as P

HEAD_DIM = 256
CONV = 4
LAYERS = 2
epsilon = 1e-06
very_negative = -1e30

VM = pl.BlockSpec(memory_space=pltpu.VMEM)
MESH = pl.DeviceIdType.MESH


def rcopy(src, dst, send, recv, axis, device):
    return pltpu.make_async_remote_copy(
        src_ref=src, dst_ref=dst, send_sem=send, recv_sem=recv,
        device_id={axis: device}, device_id_type=MESH,
    )


def bridge_kernel(ndp, ntp, steps, do_out, do_in, dense_res, lo, li, names, *refs):
    R = dict(zip(names, refs))
    f32 = jnp.float32
    bf = jnp.bfloat16
    nx = ndp // 2
    me = lax.axis_index("dp")
    core = me % 2
    x = me // 2
    partner = me + 1 - 2 * core
    z = lax.axis_index("tp")
    loads = []
    for name, layer in (("wo", lo), ("wb", li), ("wg", li)):
        if name in R:
            cp = pltpu.make_async_copy(R[name].at[layer], R[name + "_s"], R[name + "_m"])
            cp.start()
            loads.append(cp)
    barrier = pltpu.get_barrier_semaphore()
    for off in range(1, ndp):
        pl.semaphore_signal(barrier, inc=1, device_id={"dp": (me + off) % ndp}, device_id_type=MESH)
    greeted = ndp - 1
    if do_out and ntp > 1:
        @pl.when(z > 0)
        def _():
            pl.semaphore_signal(barrier, inc=1, device_id={"tp": z - 1}, device_id_type=MESH)

        @pl.when(z < ntp - 1)
        def _():
            pl.semaphore_signal(barrier, inc=1, device_id={"tp": z + 1}, device_id_type=MESH)
        greeted = greeted + jnp.where(z > 0, 1, 0) + jnp.where(z < ntp - 1, 1, 0)
    sent = []

    def start(cp):
        cp.start()
        sent.append(cp)
        return cp

    if do_out:
        m_ref, got, acc_s, sel_s, auxin = R["m"], R["got"], R["acc"], R["sel"], R["auxin"]
        chunks, piece, width = got.shape[2:]
        own = chunks * piece
        live_rows, feats = acc_s.shape
        pl.semaphore_wait(barrier, greeted)
        across = {}
        for c in range(chunks):
            for g in range(nx - 1):
                to = 2 * ((x + 1 + g) % nx) + core
                across[g, c] = start(rcopy(m_ref.at[c], got.at[x, core, c], R["ga_s"].at[g, c],
                                           R["ga_r"].at[g, c], "dp", to))
        near = start(rcopy(m_ref, got.at[x, core], R["gp_s"], R["gp_r"], "dp", partner))

        r = lax.broadcasted_iota(jnp.int32, (own, own), 0)
        c = lax.broadcasted_iota(jnp.int32, (own, own), 1)
        upper = jnp.where(r < c, 1.0, 0.0).astype(bf)
        slot = (c[0:1, :] % steps).astype(f32)
        target = lax.broadcasted_iota(jnp.int32, (live_rows, own), 0).astype(f32)
        offset = jnp.zeros((1, 1), f32)
        for d in range(ndp):
            live = jnp.where(slot < auxin[d, 1:2, :own], 1.0, 0.0)
            ahead = jnp.dot(jnp.broadcast_to(live, (8, own)).astype(bf), upper,
                            preferred_element_type=f32)[0:1, :]
            place = jnp.where(live > 0.5, ahead + offset, -1.0)
            offset = offset + jnp.sum(live, axis=1, keepdims=True)
            sel_s[d] = jnp.where(target == place, 1.0, 0.0).astype(bf)
        loads[0].wait()
        wo = R["wo_s"]

        def packed(d, rows):
            part = jnp.dot(rows, wo[...], preferred_element_type=f32).astype(bf)
            return jnp.dot(sel_s[d], part, preferred_element_type=f32)

        acc_s[...] = packed(me, m_ref[...].reshape(own, width))
        if dense_res:
            total = jnp.dot(sel_s[0], R["tok"][0], preferred_element_type=f32)
            for d in range(1, ndp):
                total = total + jnp.dot(sel_s[d], R["tok"][d], preferred_element_type=f32)
            R["res_s"][...] = total.astype(bf)
            res = R["res_s"]
        else:
            res = R["res"]
        near.wait_recv()
        acc_s[...] += packed(partner, got[x, 1 - core].reshape(own, width))
        passed = []
        for c in range(chunks):
            for g in range(nx - 1):
                origin = (x + nx - 1 - g) % nx
                across[g, c].wait_recv()
                spot = got.at[origin, core, c]
                passed.append(start(rcopy(spot, spot, R["gf_s"].at[g, c], R["gf_r"].at[g, c],
                                          "dp", partner)))
        for g in range(nx - 1):
            origin = (x + nx - 1 - g) % nx
            acc_s[...] += packed(2 * origin + core, got[origin, core].reshape(own, width))
        for cp in passed:
            cp.wait_recv()
        for g in range(nx - 1):
            origin = (x + nx - 1 - g) % nx
            acc_s[...] += packed(2 * origin + 1 - core, got[origin, 1 - core].reshape(own, width))

        xo = R["xo"]
        kz, rz = xo.shape[:2]
        half = ntp // 2
        zsum, zin, zcross = R["zsum"], R["zin"], R["zcross"]
        left = z < half
        inward = jnp.where(left, z + 1, z - 1)
        outward = jnp.where(left, z - 1, z + 1)
        edge = (z == 0) | (z == ntp - 1)
        center = (z == half - 1) | (z == half)

        def up(i):
            return rcopy(zsum.at[i], zin.at[i], R["zi_s"].at[i], R["zi_r"].at[i], "tp", inward)

        def cross(i):
            return rcopy(zsum.at[i], zcross.at[i], R["zc_s"].at[i], R["zc_r"].at[i], "tp", inward)

        def down(i):
            return rcopy(xo.at[i], xo.at[i], R["zo_s"].at[i], R["zo_r"].at[i], "tp", outward)

        def settle(i, total):
            update = total.astype(bf).astype(f32)
            xo[i] = (res[i * rz:(i + 1) * rz, :].astype(f32) + update).astype(bf)

        def mine(i):
            return acc_s[i * rz:(i + 1) * rz, :]

        def gathered(i):
            up(i).wait_recv()
            return mine(i) + zin[i].astype(f32)

        if ntp == 1:
            for i in range(kz):
                settle(i, mine(i))
        else:
            outer = jnp.logical_not(center)
            if ntp > 2:
                @pl.when(edge)
                def _():
                    for i in range(kz):
                        zsum[i] = mine(i).astype(bf)
                        up(i).start()

            if ntp > 4:
                @pl.when(outer & jnp.logical_not(edge))
                def _():
                    for i in range(kz):
                        zsum[i] = gathered(i).astype(bf)
                        up(i).start()

            if ntp > 2:
                @pl.when(outer)
                def _():
                    for i in range(kz):
                        down(i).wait_recv()
                        if ntp > 4:
                            @pl.when(jnp.logical_not(edge))
                            def _():
                                down(i).start()
                    for i in range(kz):
                        up(i).wait_send()
                        if ntp > 4:
                            @pl.when(jnp.logical_not(edge))
                            def _():
                                down(i).wait_send()

            @pl.when(center)
            def _():
                lag = 3
                for i in range(kz + lag):
                    if i < kz:
                        zsum[i] = (gathered(i) if ntp > 2 else mine(i)).astype(bf)
                        cross(i).start()
                    if i >= lag:
                        cross(i - lag).wait_recv()
                        settle(i - lag, zsum[i - lag].astype(f32) + zcross[i - lag].astype(f32))
                        if ntp > 2:
                            down(i - lag).start()
                for i in range(kz):
                    cross(i).wait_send()
                    if ntp > 2:
                        down(i).wait_send()

    def dense_rows(d):
        flat = xo[...].reshape(live_rows, feats)
        return lax.dot_general(sel_s[d], flat, (((0,), (0,)), ((), ())), preferred_element_type=f32)

    if do_in:
        ob, og, oaux, aux_s = R["ob"], R["og"], R["oaux"], R["aux_s"]
        snd, loc, r1, s2, r2 = R["snd"], R["loc"], R["r1"], R["s2"], R["r2"]
        chunks, piece, width = snd.shape[2:]
        own = chunks * piece
        r = lax.broadcasted_iota(jnp.int32, (own, own), 0)
        c = lax.broadcasted_iota(jnp.int32, (own, own), 1)
        aux_copies = []
        weights = (R["wb_s"], R["wg_s"])
        pending = list(loads[1:] if do_out else loads)

        def inner(d):
            rows = dense_rows(d) if do_out else R["tok"][d].astype(f32)
            square = jnp.sum(rows * rows, axis=1, keepdims=True)
            aux_s[d, 0:1, :own] = jnp.sum(jnp.where(r == c, square, 0.0), axis=0, keepdims=True)
            aux_s[d, 1:2, :own] = auxin[me, 1:2, :own] if do_out else R["cnt"][...]
            return (rows * R["gain"][li:li + 1, :]).astype(bf)

        def product(k, rows):
            if len(pending) > 1 - k:
                pending.pop(0).wait()
            return jnp.dot(rows, weights[k][...], preferred_element_type=f32).astype(bf)

        def tell(d, g, i):
            aux_copies.append(start(rcopy(aux_s.at[d], oaux.at[me], R["ax_s"].at[g, i],
                                          R["ax_r"].at[g, i], "dp", d)))

        first = {}
        second = {}
        for g in range(nx):
            far = (x + 1 + g) % nx
            rows = inner(2 * far + 1 - core)
            for k in range(2):
                snd[g, k] = product(k, rows).reshape(chunks, piece, width)
                if not do_out and g == 0 and k == 0:
                    pl.semaphore_wait(barrier, greeted)
                for i in range(chunks):
                    first[g, k, i] = start(rcopy(snd.at[g, k, i], r1.at[g, k, i], R["r1_s"].at[g, k, i],
                                                 R["r1_r"].at[g, k, i], "dp", partner))
            tell(2 * far + 1 - core, g, 1)
            rows = inner(2 * far + core)
            if g < nx - 1:
                tell(2 * far + core, g, 0)
            else:
                oaux[me] = aux_s[me]
            for k in range(2):
                loc[g, k] = product(k, rows).reshape(chunks, piece, width)
                if g < nx - 1:
                    for i in range(chunks):
                        first[g, k, i].wait_recv()
                        s2[g, k, i] = (loc[g, k, i].astype(f32) + r1[g, k, i].astype(f32)).astype(bf)
                        second[g, k, i] = start(rcopy(s2.at[g, k, i], r2.at[g, k, i],
                                                      R["r2_s"].at[g, k, i], R["r2_r"].at[g, k, i],
                                                      "dp", 2 * far + core))
        for k, out in ((0, ob), (1, og)):
            for i in range(chunks):
                first[nx - 1, k, i].wait_recv()
                total = loc[nx - 1, k, i].astype(f32) + r1[nx - 1, k, i].astype(f32)
                for g in range(nx - 1):
                    second[g, k, i].wait_recv()
                    total = total + r2[g, k, i].astype(f32)
                out[i] = total
        for cp in aux_copies:
            cp.wait_recv()
    else:
        result, tok = R["result"], R["tok"]
        ones = jnp.ones((live_rows, 128), bf)
        for d in range(ndp):
            hit = lax.dot_general(sel_s[d], ones, (((0,), (0,)), ((), ())), preferred_element_type=f32)
            result[d] = jnp.where(hit[:, 0:1] > 0.5, dense_rows(d).astype(bf), tok[d])
    for cp in sent:
        cp.wait_send()


def bridge(ndp, ntp, steps, own, lanes, live_rows, name, cid, lo=None, li=None, mixed=None, auxin=None,
           w_out=None, tok=None, res=None, gain=None, cnt=None, w_branch=None, w_gate=None):
    f32 = jnp.float32
    bf = jnp.bfloat16
    do_out = mixed is not None
    do_in = w_branch is not None
    nx = ndp // 2
    far = max(nx - 1, 1)
    feats = tok.shape[-1]
    width = mixed.shape[-1] if do_out else w_branch.shape[-1]
    chunks = 4 if own % 64 == 0 else 1
    piece = own // chunks
    kz = 8 if live_rows % 128 == 0 else 1
    rz = live_rows // kz
    anyspace = pl.BlockSpec(memory_space=pl.ANY)
    sem = pltpu.SemaphoreType.DMA
    names, args, specs = [], [], []

    def take(key, a, spec=VM):
        names.append(key)
        args.append(a)
        specs.append(spec)

    dense_res = do_out and res is None
    take("tok", tok)
    if do_out:
        take("m", mixed.reshape(chunks, piece, width))
        take("auxin", auxin)
        take("wo", w_out, anyspace)
        if not dense_res:
            take("res", res)
    if do_in:
        take("gain", gain)
        take("wb", w_branch, anyspace)
        take("wg", w_gate, anyspace)
        if not do_out:
            take("cnt", cnt)
    outs = []
    scratch = []

    def give(key, shape, dtype):
        names.append(key)
        outs.append(jax.ShapeDtypeStruct(shape, dtype))

    if do_out and do_in:
        give("xo", (kz, rz, feats), bf)
    if do_in:
        give("ob", (chunks, piece, width), f32)
        give("og", (chunks, piece, width), f32)
        give("oaux", (ndp, 8, lanes), f32)
    else:
        give("result", (ndp, own, feats), bf)

    def room(key, shape, dtype):
        names.append(key)
        scratch.append(pltpu.VMEM(shape, dtype))

    def sems(key, shape):
        for end in ("_s", "_r"):
            names.append(key + end)
            scratch.append(sem(shape))

    def flag(key):
        names.append(key)
        scratch.append(sem)

    if do_out:
        if not do_in:
            room("xo", (kz, rz, feats), bf)
        room("got", (nx, 2, chunks, piece, width), bf)
        room("acc", (live_rows, feats), f32)
        room("sel", (ndp, live_rows, own), bf)
        if dense_res:
            room("res_s", (live_rows, feats), bf)
        room("wo_s", w_out.shape[1:], bf)
        flag("wo_m")
        for key in ("zsum", "zin", "zcross"):
            room(key, (kz, rz, feats), bf)
        sems("ga", (far, chunks))
        sems("gf", (far, chunks))
        flag("gp_s")
        flag("gp_r")
        for key in ("zi", "zc", "zo"):
            sems(key, (kz,))
    if do_in:
        for key, a in (("wb", w_branch), ("wg", w_gate)):
            room(key + "_s", a.shape[1:], bf)
            flag(key + "_m")
        room("aux_s", (ndp, 8, lanes), f32)
        for key, groups in (("snd", nx), ("loc", nx), ("r1", nx), ("s2", far), ("r2", far)):
            room(key, (groups, 2, chunks, piece, width), bf)
        sems("r1", (nx, 2, chunks))
        sems("r2", (far, 2, chunks))
        sems("ax", (nx, 2))
    return pl.pallas_call(
        functools.partial(bridge_kernel, ndp, ntp, steps, do_out, do_in, dense_res, lo, li, names),
        out_shape=tuple(outs),
        in_specs=specs,
        out_specs=(VM,) * len(outs),
        scratch_shapes=scratch,
        compiler_params=pltpu.CompilerParams(collective_id=cid, has_side_effects=True),
        name=name,
    )(*args)


def cell_kernel(layer, model, heads, steps, cnt_ref, bi_ref, bf_ref, br_ref, gt_ref, aux_ref,
                ccol_ref, crow_ref, mcol_ref, st_ref, cw_ref, wq_ref, wk_ref, wv_ref, wg_ref,
                og_ref, sg_ref, mem_ref, *rest):
    (mixed_ref, nc_ref, newmem_ref, nmax_ref,
     pad_s, conv_s, q_s, k_s, v_s, num_s, car_s, dec_s, cs_s, top_s, nc_s, stage, ins, outs) = rest[-18:]
    f32 = jnp.float32
    bf = jnp.bfloat16
    batch = stage.shape[0]
    own, width = br_ref.shape
    dim = HEAD_DIM
    base = 8 - (CONV - 1)

    def fetch(b):
        return pltpu.make_async_copy(mem_ref.at[layer, b], stage.at[b], ins.at[b])

    def store(b):
        return pltpu.make_async_copy(stage.at[b], newmem_ref.at[layer, b], outs.at[b])

    for b in range(batch):
        fetch(b).start()

    squares = aux_ref[0, 0:1, :own]
    for i in range(1, aux_ref.shape[0]):
        squares = squares + aux_ref[i, 0:1, :own]
    inv_row = lax.rsqrt(squares / model + epsilon)
    r = lax.broadcasted_iota(jnp.int32, (own, own), 0)
    c = lax.broadcasted_iota(jnp.int32, (own, own), 1)
    inv = jnp.sum(jnp.where(r == c, inv_row, 0.0), axis=1, keepdims=True)
    branch = (br_ref[...] * inv).astype(bf)
    pad_s[:, 8:8 + steps, :] = branch.astype(f32).reshape(batch, steps, width)
    for j in range(CONV - 1):
        rows = st_ref[0, j].astype(f32)
        for b in range(batch):
            pad_s[b, base + j:base + j + 1, :] = rows[b:b + 1, :]
    total = pad_s[:, base:base + steps, :] * cw_ref[0, 0:1, :]
    for j in range(1, CONV):
        total = total + pad_s[:, base + j:base + j + steps, :] * cw_ref[0, j:j + 1, :]
    conv = (total * jax.nn.sigmoid(total)).astype(bf).reshape(own, width)
    conv_s[...] = conv
    for b in range(batch):
        for i in range(CONV - 1):
            nc_s[i, b:b + 1, :] = pad_s[b, pl.ds(base + i + cnt_ref[b], 1), :]
    nc_ref[...] = nc_s[...].astype(bf)

    same = (r // steps) == (c // steps)
    causal = same & (r >= c)
    behind = same & (r <= c)
    live_col = (r[:, 0:1] % steps) < ccol_ref[...]
    live_row = (c[0:1, :] % steps) < crow_ref[...]
    nt = (((1,), (1,)), ((), ()))
    for h in range(heads):
        sl = slice(h * dim, (h + 1) * dim)
        q = jnp.dot(conv[:, sl], wq_ref[0, h], preferred_element_type=f32).astype(bf)
        k = jnp.dot(conv[:, sl], wk_ref[0, h], preferred_element_type=f32).astype(bf)
        v = jnp.dot(branch[:, sl], wv_ref[0, h], preferred_element_type=f32).astype(bf)
        gcol = None
        for i, part in enumerate((q, k, v)):
            w = wg_ref[0, h, :, i * dim:(i + 1) * dim]
            one = lax.dot_general(part, w, nt, preferred_element_type=f32)
            two = lax.dot_general(w, part, nt, preferred_element_type=f32)
            gcol, grow = (one, two) if gcol is None else (gcol + one, grow + two)
        bias_i = bi_ref[layer, h]
        bias_f = bf_ref[layer, h]

        def log_sig(x):
            return jnp.minimum(x, 0.0) - jnp.log1p(jnp.exp(-jnp.abs(x)))

        ig_col = jnp.where(live_col, gcol[:, 0:1] + bias_i, very_negative)
        ig_row = jnp.where(live_row, grow[0:1, :] + bias_i, very_negative)
        fg_col = jnp.where(live_col, log_sig(gcol[:, 1:2] + bias_f), 0.0)
        fg_row = jnp.where(live_row, log_sig(grow[1:2, :] + bias_f), 0.0)
        cum_col = jnp.sum(jnp.where(causal, fg_row, 0.0), axis=1, keepdims=True)
        end_col = jnp.sum(jnp.where(same, fg_row, 0.0), axis=1, keepdims=True)
        cum_row = jnp.sum(jnp.where(behind, fg_col, 0.0), axis=0, keepdims=True)
        lift_row = ig_row - cum_row
        logw = jnp.where(causal, cum_col + lift_row, very_negative)
        old_max = mcol_ref[:, h:h + 1]
        carried = cum_col + old_max
        stab = jnp.maximum(jnp.max(logw, axis=1, keepdims=True), carried)
        weights = jnp.exp(logw - stab)
        top = jnp.max(jnp.where(same, end_col + lift_row, very_negative), axis=1, keepdims=True)
        new_max = jnp.maximum(top, end_col + old_max)
        update = jnp.exp(end_col - cum_col + ig_col - new_max)
        top_s[:, h:h + 1] = new_max
        dec_s[:, h:h + 1] = jnp.exp(end_col + old_max - new_max)
        cs_s[:, h:h + 1] = jnp.exp(carried - stab)
        scores = lax.dot_general(q, k, nt, preferred_element_type=f32)
        scores = (jnp.where(causal, scores, 0.0) * (dim ** -0.5) * weights).astype(bf)
        num_s[:, sl] = jnp.dot(scores, v, preferred_element_type=f32)
        q_s[:, sl] = q.astype(f32)
        k_s[:, sl] = k.astype(f32) * (dim ** -0.5) * update
        v_s[:, sl] = v.astype(f32)
    nmax_ref[...] = top_s[pl.ds(steps - 1, batch, stride=steps), :]

    @pl.loop(0, batch)
    def _(b):
        fetch(b).wait()
        rows = pl.ds(pl.multiple_of(b * steps, 8), steps)
        for h in range(heads):
            sl = slice(h * dim, (h + 1) * dim)
            old = stage[b, h]
            car_s[rows, sl] = jnp.dot(q_s[rows, sl].astype(bf), old.astype(bf), preferred_element_type=f32)
            outer = lax.dot_general(
                k_s[rows, sl].astype(bf), v_s[rows, sl].astype(bf), (((0,), (0,)), ((), ())),
                preferred_element_type=f32,
            )
            stage[b, h] = dec_s[rows, :][0:1, h:h + 1] * old + outer
        store(b).start()

    live = (lax.broadcasted_iota(jnp.int32, (own, 1), 0) % steps) < ccol_ref[...]
    for h in range(heads):
        sl = slice(h * dim, (h + 1) * dim)
        num = num_s[:, sl] + cs_s[:, h:h + 1] * car_s[:, sl]
        centered = num - jnp.mean(num, axis=1, keepdims=True)
        normal = centered * lax.rsqrt(jnp.mean(centered * centered, axis=1, keepdims=True) + epsilon)
        gate = (gt_ref[:, sl] * inv).astype(bf).astype(f32)
        mixed = normal * og_ref[0, h:h + 1, :] + sg_ref[layer:layer + 1, sl] * conv_s[:, sl].astype(f32)
        mixed = mixed * (gate * jax.nn.sigmoid(gate))
        mixed_ref[:, sl] = jnp.where(live, mixed, 0.0).astype(bf)
    for b in range(batch):
        store(b).wait()


def memory_cell(layer, model, steps, counts, bias_input, bias_forget, branch, gate, aux, count_col,
                count_row, old_max, state, conv_weight, w_query, w_key, w_value, w_gates, out_gain,
                skip_gain, memory, previous):
    _, batch, heads, dim, _ = memory.shape
    own, width = branch.shape
    f32 = jnp.float32

    def whole(a):
        return pl.BlockSpec(a.shape, lambda i: (0,) * a.ndim)

    def layered(a):
        return pl.BlockSpec((1,) + a.shape[1:], lambda i: (layer,) + (0,) * (a.ndim - 1))

    smem = pl.BlockSpec(memory_space=pltpu.SMEM)
    anyspace = pl.BlockSpec(memory_space=pl.ANY)
    args = [counts, bias_input, bias_forget, branch, gate, aux, count_col, count_row, old_max,
            state, conv_weight, w_query, w_key, w_value, w_gates, out_gain, skip_gain, memory]
    specs = [smem, smem, smem] + [whole(a) for a in args[3:9]] + [layered(a) for a in args[9:16]]
    specs += [whole(skip_gain), anyspace]
    aliases = {}
    if previous is not None:
        aliases = {len(args): 2}
        args.append(previous)
        specs.append(anyspace)
    big = pltpu.VMEM((own, width), f32)
    small = pltpu.VMEM((own, 128), f32)
    return pl.pallas_call(
        functools.partial(cell_kernel, layer, model, heads, steps),
        grid=(1,),
        out_shape=(
            jax.ShapeDtypeStruct((own, width), jnp.bfloat16),
            jax.ShapeDtypeStruct((CONV - 1, batch, width), jnp.bfloat16),
            jax.ShapeDtypeStruct(memory.shape, f32),
            jax.ShapeDtypeStruct((batch, 128), f32),
        ),
        in_specs=specs,
        out_specs=(
            pl.BlockSpec((own, width), lambda i: (0, 0)),
            pl.BlockSpec((CONV - 1, batch, width), lambda i: (0, 0, 0)),
            anyspace,
            pl.BlockSpec((batch, 128), lambda i: (0, 0)),
        ),
        scratch_shapes=[
            pltpu.VMEM((batch, 8 + steps, width), f32),
            pltpu.VMEM((own, width), jnp.bfloat16),
            big, big, big, big, big, small, small, small,
            pltpu.VMEM((CONV - 1, batch, width), f32),
            pltpu.VMEM((batch, heads, dim, dim), f32),
            pltpu.SemaphoreType.DMA((batch,)), pltpu.SemaphoreType.DMA((batch,)),
        ],
        input_output_aliases=aliases,
        compiler_params=pltpu.CompilerParams(dimension_semantics=("arbitrary",)),
        name="memory_cell",
    )(*args)


def per_device(tokens, live_counts, norm_gain, w_branch, w_silu_gate, conv_weight, w_query, w_key,
               w_value, w_input_gate, w_forget_gate, bias_input, bias_forget, out_gain, skip_gain,
               w_out, conv_state, memory, max_state):
    f32 = jnp.float32
    ndp = lax.axis_size("dp")
    ntp = lax.axis_size("tp")
    all_batch, steps, features = tokens.shape
    batch = live_counts.shape[0]
    width = w_branch.shape[2]
    heads = w_query.shape[1]
    own = batch * steps
    live_rows = all_batch * steps // 2
    lanes = -(-own // 128) * 128
    model = features * ndp
    flat = tokens.reshape(ndp, own, features)
    repeated = jnp.repeat(live_counts, steps)
    count_col = repeated[:, None]
    count_row = repeated[None, :]
    old_max = jnp.repeat(max_state, steps, axis=1)
    states = jnp.transpose(conv_state, (0, 2, 1, 3))
    w_gates = jnp.pad(jnp.stack([w_input_gate, w_forget_gate], axis=2), ((0, 0), (0, 0), (0, 6), (0, 0)))
    link = functools.partial(bridge, ndp, ntp, steps, own, lanes, live_rows)

    branch, gate, aux = link("enter", 0, li=0, tok=flat, gain=norm_gain, cnt=count_row.astype(f32),
                             w_branch=w_branch, w_gate=w_silu_gate)
    new_memory = None
    compact = None
    conv_list = []
    max_list = []
    for l in range(LAYERS):
        mixed, new_conv, new_memory, new_max = memory_cell(
            l, model, steps, live_counts, bias_input, bias_forget, branch.reshape(own, width),
            gate.reshape(own, width), aux, count_col, count_row, old_max[l], states, conv_weight,
            w_query, w_key, w_value, w_gates, out_gain, skip_gain, memory, new_memory
        )
        conv_list.append(new_conv)
        max_list.append(new_max[:, :heads])
        if l + 1 < LAYERS:
            compact, branch, gate, aux = link(
                f"bridge{l}", l + 1, lo=l, li=l + 1, mixed=mixed, auxin=aux, w_out=w_out, tok=flat,
                res=compact, gain=norm_gain, w_branch=w_branch, w_gate=w_silu_gate
            )
            compact = compact.reshape(live_rows, features)
        else:
            (result,) = link("leave", l + 1, lo=l, mixed=mixed, auxin=aux, w_out=w_out, tok=flat, res=compact)
    new_conv = jnp.transpose(jnp.stack(conv_list), (0, 2, 1, 3))
    return (result.reshape(tokens.shape), new_conv, new_memory, jnp.stack(max_list))


def solution(mesh):
    in_specs = (
        P("grp", None, "dp"),
        P(("grp", "dp")),
        P(None, "dp"),
        P(None, "dp", "tp"),
        P(None, "dp", "tp"),
        P(None, None, "tp"),
        P(None, "tp", None, None),
        P(None, "tp", None, None),
        P(None, "tp", None, None),
        P(None, "tp", None),
        P(None, "tp", None),
        P(None, "tp"),
        P(None, "tp"),
        P(None, "tp", None),
        P(None, "tp"),
        P(None, "tp", "dp"),
        P(None, ("grp", "dp"), None, "tp"),
        P(None, ("grp", "dp"), "tp", None, None),
        P(None, ("grp", "dp"), "tp"),
    )
    out_specs = (
        P("grp", None, "dp"),
        P(None, ("grp", "dp"), None, "tp"),
        P(None, ("grp", "dp"), "tp", None, None),
        P(None, ("grp", "dp"), "tp"),
    )
    return jax.shard_map(
        per_device, mesh=mesh, in_specs=in_specs, out_specs=out_specs, check_vma=False
    )
```

```python
import functools

import jax
import jax.numpy as jnp
from jax import lax
from jax.experimental import pallas as pl
from jax.experimental.pallas import tpu as pltpu
from jax.sharding import PartitionSpec as P

HEAD_DIM = 256
CONV = 4
LAYERS = 2
epsilon = 1e-06
very_negative = -1e30

FULL_VMEM = 60 * 1024 * 1024
LEAVE_VMEM = 24 * 1024 * 1024

VM = pl.BlockSpec(memory_space=pltpu.VMEM)
MESH = pl.DeviceIdType.MESH


def rcopy(src, dst, send, recv, axis, device):
    return pltpu.make_async_remote_copy(
        src_ref=src, dst_ref=dst, send_sem=send, recv_sem=recv,
        device_id={axis: device}, device_id_type=MESH,
    )


def bridge_kernel(ndp, ntp, do_out, do_in, lo, li, names, *refs):
    R = dict(zip(names, refs))
    f32 = jnp.float32
    bf = jnp.bfloat16
    nx = ndp // 2
    me = lax.axis_index("dp")
    core = me % 2
    x = me // 2
    partner = me + 1 - 2 * core
    z = lax.axis_index("tp")
    tok = R["tok"]
    chunks, piece, feats = tok.shape[1:]
    own = chunks * piece
    halves = 2 if chunks > 1 else 1
    step = chunks // halves
    pieces = {}
    for h in range(halves):
        pieces[h] = list(range(h * step, (h + 1) * step))

    def load(name, layer):
        return pltpu.make_async_copy(R[name].at[layer], R[name + "_s"], R[name + "_m"])

    wanted = ([("wo", lo)] if do_out else []) + ([("wb", li), ("wg", li)] if do_in else [])
    for name, layer in wanted:
        load(name, layer).start()
    barrier = pltpu.get_barrier_semaphore()
    for off in range(1, ndp):
        pl.semaphore_signal(barrier, inc=1, device_id={"dp": (me + off) % ndp}, device_id_type=MESH)
    greeted = ndp - 1
    if do_out and ntp > 1:
        @pl.when(z > 0)
        def _():
            pl.semaphore_signal(barrier, inc=1, device_id={"tp": z - 1}, device_id_type=MESH)

        @pl.when(z < ntp - 1)
        def _():
            pl.semaphore_signal(barrier, inc=1, device_id={"tp": z + 1}, device_id_type=MESH)
        greeted = greeted + jnp.where(z > 0, 1, 0) + jnp.where(z < ntp - 1, 1, 0)
    pl.semaphore_wait(barrier, greeted)

    def ahead(g):
        return (x + 1 + g) % nx

    def behind(g):
        return (x + nx - 1 - g) % nx

    groups = [("mine", nx - 1, h) for h in range(halves)]
    groups += [("other", nx - 1, 0)]
    for g in range(nx - 1):
        for h in range(halves):
            groups += [("mine", g, h), ("other", g, h)]
    groups += [("other", nx - 1, h) for h in range(1, halves)]
    if not do_out:
        groups = [(kind, g, h) for g in range(nx) for h in range(halves) for kind in ("other", "mine")]

    if do_out:
        m_ref, got, psum = R["m"], R["got"], R["psum"]
        width = m_ref.shape[2]
        fresh = R["fresh"]

        def device(kind, g):
            if g == nx - 1:
                return me if kind == "mine" else partner
            return 2 * behind(g) + (core if kind == "mine" else 1 - core)

        def across(g, c):
            return rcopy(m_ref.at[c], got.at[x, core, c], R["ga_s"].at[g, c], R["ga_r"].at[g, c],
                         "dp", 2 * ahead(g) + core)

        def near(c):
            return rcopy(m_ref.at[c], got.at[x, core, c], R["gp_s"].at[c], R["gp_r"].at[c],
                         "dp", partner)

        def passed(g, c):
            spot = got.at[behind(g), core, c]
            return rcopy(spot, spot, R["gf_s"].at[g, c], R["gf_r"].at[g, c], "dp", partner)

        for c in range(chunks):
            for g in range(nx - 1):
                across(g, c).start()
        for c in range(chunks):
            near(c).start()
        load("wo", lo).wait()

        def rows_of(kind, g, h):
            if g == nx - 1:
                if kind == "mine":
                    return m_ref[h * step:(h + 1) * step]
                for c in pieces[h]:
                    near(c).wait_recv()
                return got[x, 1 - core, h * step:(h + 1) * step]
            if kind == "mine":
                for c in pieces[h]:
                    across(g, c).wait_recv()
                    passed(g, c).start()
                return got[behind(g), core, h * step:(h + 1) * step]
            for c in pieces[h]:
                passed(g, c).wait_recv()
            return got[behind(g), 1 - core, h * step:(h + 1) * step]

        def product_out(i):
            rows = rows_of(*groups[i]).reshape(step * piece, width)
            part = jnp.dot(rows, R["wo_s"][...], preferred_element_type=f32)
            psum[i * step:(i + 1) * step] = part.reshape(step, piece, feats)

        half = ntp // 2
        zsum, zin, zcross = R["zsum"], R["zin"], R["zcross"]
        left = z < half
        inward = jnp.where(left, z + 1, z - 1)
        outward = jnp.where(left, z - 1, z + 1)
        edge = (z == 0) | (z == ntp - 1)
        center = (z == half - 1) | (z == half)
        inner = jnp.logical_not(edge)
        outer = jnp.logical_not(center)
        spots = len(groups) * step

        def spot_of(p):
            kind, g, h = groups[p // step]
            return device(kind, g), h * step + p % step

        def up(p):
            return rcopy(zsum.at[p], zin.at[p], R["zi_s"].at[p], R["zi_r"].at[p], "tp", inward)

        def cross(p):
            return rcopy(zsum.at[p], zcross.at[p], R["zc_s"].at[p], R["zc_r"].at[p], "tp", inward)

        def down(p):
            d, c = spot_of(p)
            return rcopy(fresh.at[d, c], fresh.at[d, c], R["zo_s"].at[p], R["zo_r"].at[p], "tp", outward)

        def settle(p, total):
            d, c = spot_of(p)
            update = total.astype(bf).astype(f32)
            fresh[d, c] = (tok[d, c].astype(f32) + update).astype(bf)

        def gathered(p):
            up(p).wait_recv()
            return psum[p] + zin[p].astype(f32)

    if do_in:
        ob, og, oaux, aux_s = R["ob"], R["og"], R["oaux"], R["aux_s"]
        snd, loc, r1, s2, r2 = R["snd"], R["loc"], R["r1"], R["s2"], R["r2"]
        wide = snd.shape[-1]
        weights = (R["wb_s"], R["wg_s"])
        source = fresh if do_out else tok
        aux_s[...] = jnp.zeros_like(aux_s)

        def target(kind, g):
            if g == nx - 1:
                return me if kind == "mine" else partner
            return 2 * ahead(g) + (core if kind == "mine" else 1 - core)

        def first(g, k, c):
            return rcopy(snd.at[g, k, c], r1.at[g, k, c], R["r1_s"].at[g, k, c], R["r1_r"].at[g, k, c],
                         "dp", partner)

        def second(g, k, c):
            return rcopy(s2.at[g, k, c], r2.at[g, k, c], R["r2_s"].at[g, k, c], R["r2_r"].at[g, k, c],
                         "dp", 2 * ahead(g) + core)

        def tell(kind, g):
            d = target(kind, g)
            i = 0 if kind == "mine" else 1
            return rcopy(aux_s.at[d], oaux.at[me], R["ax_s"].at[g, i], R["ax_r"].at[g, i], "dp", d)

        def forward(g, h):
            for k in range(2):
                for c in pieces[h]:
                    first(g, k, c).wait_recv()
                    s2[g, k, c] = (loc[g, k, c].astype(f32) + r1[g, k, c].astype(f32)).astype(bf)
                    second(g, k, c).start()

        def handle(kind, g, h, done, waiting):
            gw = g
            if do_out and g < nx - 1:
                gw = nx - 2 - g
            d = target(kind, gw)
            size = step * piece
            rows = source[d, h * step:(h + 1) * step].reshape(size, feats).astype(f32)
            square = jnp.sum(rows * rows, axis=1, keepdims=True)
            r = lax.broadcasted_iota(jnp.int32, (size, own), 0) + h * size
            c = lax.broadcasted_iota(jnp.int32, (size, own), 1)
            line = jnp.sum(jnp.where(r == c, square, 0.0), axis=0, keepdims=True)
            if h == 0:
                aux_s[d, 0:1, :own] = line
            else:
                aux_s[d, 0:1, :own] += line
            done.append((kind, gw))
            scaled = (rows * R["gain"][li:li + 1, :]).astype(bf)
            for k in range(2):
                part = jnp.dot(scaled, weights[k][...], preferred_element_type=f32).astype(bf)
                part = part.reshape(step, piece, wide)
                if kind == "mine":
                    loc[gw, k, h * step:(h + 1) * step] = part
                else:
                    snd[gw, k, h * step:(h + 1) * step] = part
                    for c in pieces[h]:
                        first(gw, k, c).start()
            if done.count((kind, gw)) == halves:
                if (kind, gw) == ("mine", nx - 1):
                    oaux[me] = aux_s[me]
                else:
                    tell(kind, gw).start()
            while waiting:
                forward(*waiting.pop(0))
            if gw < nx - 1:
                pair = [(a, gw, h) for a in ("mine", "other")]
                done.append(("seen", kind, gw, h))
                if all(("seen",) + a in done for a in pair):
                    waiting.append((gw, h))

        def flush(waiting):
            while waiting:
                forward(*waiting.pop(0))

    if do_in:
        for name in ("wb", "wg"):
            load(name, li).wait()
    if not do_out:
        done, waiting = [], []
        for group in groups:
            handle(*group, done, waiting)
        flush(waiting)
    else:
        def finish(i, done, waiting):
            if do_in:
                handle(*groups[i], done, waiting)

        if ntp == 1:
            done, waiting = [], []
            for i in range(len(groups)):
                product_out(i)
                for p in range(i * step, (i + 1) * step):
                    settle(p, psum[p])
                finish(i, done, waiting)
            if do_in:
                flush(waiting)
        else:
            if ntp > 2:
                @pl.when(outer)
                def _():
                    done, waiting = [], []
                    for i in range(len(groups)):
                        product_out(i)
                        for p in range(i * step, (i + 1) * step):
                            if ntp == 4:
                                zsum[p] = psum[p].astype(bf)
                            else:
                                @pl.when(edge)
                                def _():
                                    zsum[p] = psum[p].astype(bf)

                                @pl.when(inner)
                                def _():
                                    zsum[p] = gathered(p).astype(bf)
                            up(p).start()
                    for i in range(len(groups)):
                        for p in range(i * step, (i + 1) * step):
                            down(p).wait_recv()
                            if ntp > 4:
                                @pl.when(inner)
                                def _():
                                    down(p).start()
                        finish(i, done, waiting)
                    if do_in:
                        flush(waiting)
                    for p in range(spots):
                        up(p).wait_send()
                        if ntp > 4:
                            @pl.when(inner)
                            def _():
                                down(p).wait_send()

            @pl.when(center)
            def _():
                done, waiting = [], []
                lag = 3
                for p in range(spots + lag):
                    if p < spots:
                        if p % step == 0:
                            product_out(p // step)
                        zsum[p] = (gathered(p) if ntp > 2 else psum[p]).astype(bf)
                        cross(p).start()
                    q = p - lag
                    if q >= 0:
                        cross(q).wait_recv()
                        settle(q, zsum[q].astype(f32) + zcross[q].astype(f32))
                        if ntp > 2:
                            down(q).start()
                        if q % step == step - 1:
                            finish(q // step, done, waiting)
                if do_in:
                    flush(waiting)
                for p in range(spots):
                    cross(p).wait_send()
                    if ntp > 2:
                        down(p).wait_send()

        for c in range(chunks):
            near(c).wait_send()
            for g in range(nx - 1):
                across(g, c).wait_send()
                passed(g, c).wait_send()

    if do_in:
        last = nx - 1
        for g in range(nx):
            for i, kind in enumerate(("mine", "other")):
                if (kind, g) != ("mine", last):
                    tell(kind, g).wait_recv()
        total = oaux[0, 0:1, :own]
        for d in range(1, ndp):
            total = total + oaux[d, 0:1, :own]
        inv_row = lax.rsqrt(total / (feats * ndp) + epsilon)
        r = lax.broadcasted_iota(jnp.int32, (own, own), 0)
        c = lax.broadcasted_iota(jnp.int32, (own, own), 1)
        inv = jnp.sum(jnp.where(r == c, inv_row, 0.0), axis=1, keepdims=True)
        for h in range(halves):
            for k, out in ((0, ob), (1, og)):
                for c in pieces[h]:
                    first(last, k, c).wait_recv()
                    total = loc[last, k, c].astype(f32) + r1[last, k, c].astype(f32)
                    for g in range(nx - 1):
                        second(g, k, c).wait_recv()
                        total = total + r2[g, k, c].astype(f32)
                    out[c * piece:(c + 1) * piece, :] = (
                        total * inv[c * piece:(c + 1) * piece, :]
                    ).astype(bf)
        for g in range(nx):
            for kind in ("mine", "other"):
                if (kind, g) != ("mine", last):
                    tell(kind, g).wait_send()
            for k in range(2):
                for c in range(chunks):
                    first(g, k, c).wait_send()
                    if g < last:
                        second(g, k, c).wait_send()


def bridge(ndp, ntp, lanes, name, cid, limit, tok, lo=None, li=None, mixed=None, w_out=None, gain=None,
           w_branch=None, w_gate=None):
    f32 = jnp.float32
    bf = jnp.bfloat16
    do_out = mixed is not None
    do_in = w_branch is not None
    nx = ndp // 2
    far = max(nx - 1, 1)
    chunks, piece, feats = tok.shape[1:]
    own = chunks * piece
    spots = ndp * chunks
    weight = pl.BlockSpec(memory_space=pl.ANY)
    sem = pltpu.SemaphoreType.DMA
    names, args, specs, outs, scratch = [], [], [], [], []

    def take(key, a, spec=VM):
        names.append(key)
        args.append(a)
        specs.append(spec)

    take("tok", tok)
    if do_out:
        width = mixed.shape[-1]
        take("m", mixed.reshape(chunks, piece, width))
        take("wo", w_out, weight)
    if do_in:
        width = w_branch.shape[-1]
        take("gain", gain)
        take("wb", w_branch, weight)
        take("wg", w_gate, weight)

    def give(key, shape, dtype):
        names.append(key)
        outs.append(jax.ShapeDtypeStruct(shape, dtype))

    if do_out:
        give("fresh", tok.shape, bf)
    if do_in:
        give("ob", (own, width), bf)
        give("og", (own, width), bf)

    def room(key, shape, dtype):
        names.append(key)
        scratch.append(pltpu.VMEM(shape, dtype))

    def flag(key, *shape):
        names.append(key)
        scratch.append(sem(shape) if shape else sem)

    def sems(key, *shape):
        flag(key + "_s", *shape)
        flag(key + "_r", *shape)

    if do_out:
        room("got", (nx, 2, chunks, piece, width), bf)
        room("psum", (spots, piece, feats), f32)
        room("wo_s", w_out.shape[1:], bf)
        flag("wo_m")
        for key in ("zsum", "zin", "zcross"):
            room(key, (spots, piece, feats), bf)
        sems("ga", far, chunks)
        sems("gf", far, chunks)
        sems("gp", chunks)
        for key in ("zi", "zc", "zo"):
            sems(key, spots)
    if do_in:
        for key, a in (("wb", w_branch), ("wg", w_gate)):
            room(key + "_s", a.shape[1:], bf)
            flag(key + "_m")
        room("aux_s", (ndp, 8, lanes), f32)
        room("oaux", (ndp, 8, lanes), f32)
        for key, count in (("snd", nx), ("loc", nx), ("r1", nx), ("s2", far), ("r2", far)):
            room(key, (count, 2, chunks, piece, width), bf)
        sems("r1", nx, 2, chunks)
        sems("r2", far, 2, chunks)
        sems("ax", nx, 2)
    return pl.pallas_call(
        functools.partial(bridge_kernel, ndp, ntp, do_out, do_in, lo, li, names),
        out_shape=tuple(outs),
        in_specs=specs,
        out_specs=(VM,) * len(outs),
        scratch_shapes=scratch,
        compiler_params=pltpu.CompilerParams(
            collective_id=cid, has_side_effects=True, vmem_limit_bytes=limit
        ),
        name=name,
    )(*args)


def cell_kernel(layer, heads, steps, cnt_ref, bi_ref, bf_ref, cvec_ref, br_ref, gt_ref, mrow_ref, st_ref,
                cw_ref, wi_ref, wf_ref, og_ref, sg_ref, wq_ref, wk_ref, wv_ref, mem_ref, *rest):
    (mixed_ref, nc_ref, newmem_ref, nmax_ref,
     pad_s, conv_s, q_s, k_s, v_s, num_s, car_s, dec_s, cs_s, nc_s, w_s, stage, ins, outs,
     w_sem) = rest[-19:]
    f32 = jnp.float32
    bf = jnp.bfloat16
    batch = stage.shape[0]
    own, width = br_ref.shape
    dim = HEAD_DIM
    base = 8 - (CONV - 1)

    def fetch(b):
        return pltpu.make_async_copy(mem_ref.at[layer, b], stage.at[b], ins.at[b])

    def store(b):
        return pltpu.make_async_copy(stage.at[b], newmem_ref.at[layer, b], outs.at[b])

    maps = [
        pltpu.make_async_copy(w_ref.at[layer], w_s.at[i], w_sem.at[i])
        for i, w_ref in enumerate((wq_ref, wk_ref, wv_ref))
    ]
    for cp in maps:
        cp.start()

    @pl.loop(0, batch)
    def _(b):
        fetch(b).start()

    r = lax.broadcasted_iota(jnp.int32, (own, own), 0)
    c = lax.broadcasted_iota(jnp.int32, (own, own), 1)
    row = lax.broadcasted_iota(jnp.int32, (own, batch), 0)
    seq = lax.broadcasted_iota(jnp.int32, (own, batch), 1)
    belongs = (row // steps) == seq
    closing = row == seq * steps + (steps - 1)
    nt = (((1,), (1,)), ((), ()))
    spread = jnp.where(belongs, 1.0, 0.0)
    counts = jnp.broadcast_to(cvec_ref[...].astype(f32), (8, batch))
    count_row = lax.dot_general(counts, spread, nt, preferred_element_type=f32)[0:1, :]
    count_col = jnp.sum(jnp.where(belongs, counts[0:1, :], 0.0), axis=1, keepdims=True)
    branch = br_ref[...]
    pad_s[:, 8:8 + steps, :] = branch.astype(f32).reshape(batch, steps, width)
    for j in range(CONV - 1):
        rows = st_ref[layer, j].astype(f32)
        for b in range(batch):
            pad_s[b, base + j:base + j + 1, :] = rows[b:b + 1, :]
    total = pad_s[:, base:base + steps, :] * cw_ref[layer, 0:1, :]
    for j in range(1, CONV):
        total = total + pad_s[:, base + j:base + j + steps, :] * cw_ref[layer, j:j + 1, :]
    conv = (total * jax.nn.sigmoid(total)).astype(bf).reshape(own, width)
    conv_s[...] = conv
    for b in range(batch):
        for i in range(CONV - 1):
            nc_s[i, b:b + 1, :] = pad_s[b, pl.ds(base + i + cnt_ref[b], 1), :]
    nc_ref[layer] = nc_s[...].astype(bf)
    for l in range(nc_ref.shape[0]):
        if l != layer and len(rest) > 19:
            nc_ref[l] = rest[1][l]
            nmax_ref[l] = rest[2][l]
        elif l != layer:
            nc_ref[l] = jnp.zeros_like(nc_ref[l])
            nmax_ref[l] = jnp.zeros_like(nmax_ref[l])

    same = (r // steps) == (c // steps)
    causal = same & (r >= c)
    behind = same & (r <= c)
    live_col = (r[:, 0:1] % steps).astype(f32) < count_col
    live_row = (c[0:1, :] % steps).astype(f32) < count_row
    for cp in maps:
        cp.wait()
    for h in range(heads):
        sl = slice(h * dim, (h + 1) * dim)
        q = jnp.dot(conv[:, sl], w_s[0, h], preferred_element_type=f32).astype(bf)
        k = jnp.dot(conv[:, sl], w_s[1, h], preferred_element_type=f32).astype(bf)
        v = jnp.dot(branch[:, sl], w_s[2, h], preferred_element_type=f32).astype(bf)
        cols = []
        rows = []
        for g_ref in (wi_ref, wf_ref):
            col = None
            for i, part in enumerate((q, k, v)):
                w = g_ref[layer, :, i * dim:(i + 1) * dim]
                if heads == 1:
                    w = jnp.broadcast_to(w.astype(f32), (8, dim)).astype(bf)
                one = lax.dot_general(part, w, nt, preferred_element_type=f32)
                two = lax.dot_general(w, part, nt, preferred_element_type=f32)
                col, line = (one, two) if col is None else (col + one, line + two)
            cols.append(col[:, h:h + 1])
            rows.append(line[h:h + 1, :])
        bias_i = bi_ref[layer, h]
        bias_f = bf_ref[layer, h]

        def log_sig(x):
            return jnp.minimum(x, 0.0) - jnp.log1p(jnp.exp(-jnp.abs(x)))

        ig_col = jnp.where(live_col, cols[0] + bias_i, very_negative)
        ig_row = jnp.where(live_row, rows[0] + bias_i, very_negative)
        fg_col = jnp.where(live_col, log_sig(cols[1] + bias_f), 0.0)
        fg_row = jnp.where(live_row, log_sig(rows[1] + bias_f), 0.0)
        cum_col = jnp.sum(jnp.where(causal, fg_row, 0.0), axis=1, keepdims=True)
        end_col = jnp.sum(jnp.where(same, fg_row, 0.0), axis=1, keepdims=True)
        cum_row = jnp.sum(jnp.where(behind, fg_col, 0.0), axis=0, keepdims=True)
        lift_row = ig_row - cum_row
        logw = jnp.where(causal, cum_col + lift_row, very_negative)
        old_max = jnp.sum(jnp.where(belongs, mrow_ref[layer, h:h + 1, :], 0.0), axis=1, keepdims=True)
        carried = cum_col + old_max
        stab = jnp.maximum(jnp.max(logw, axis=1, keepdims=True), carried)
        weights = jnp.exp(logw - stab)
        top = jnp.max(jnp.where(same, end_col + lift_row, very_negative), axis=1, keepdims=True)
        new_max = jnp.maximum(top, end_col + old_max)
        update = jnp.exp(end_col - cum_col + ig_col - new_max)
        nmax_ref[layer, h:h + 1, :] = jnp.sum(jnp.where(closing, new_max, 0.0), axis=0, keepdims=True)
        dec_s[:, h:h + 1] = jnp.exp(end_col + old_max - new_max)
        cs_s[:, h:h + 1] = jnp.exp(carried - stab)
        scores = lax.dot_general(q, k, nt, preferred_element_type=f32)
        scores = (jnp.where(causal, scores, 0.0) * (dim ** -0.5) * weights).astype(bf)
        num_s[:, sl] = jnp.dot(scores, v, preferred_element_type=f32)
        q_s[:, sl] = q.astype(f32)
        k_s[:, sl] = k.astype(f32) * (dim ** -0.5) * update
        v_s[:, sl] = v.astype(f32)

    @pl.loop(0, batch)
    def _(b):
        fetch(b).wait()
        rows = pl.ds(pl.multiple_of(b * steps, 8), steps)
        for h in range(heads):
            sl = slice(h * dim, (h + 1) * dim)
            old = stage[b, h]
            car_s[rows, sl] = jnp.dot(q_s[rows, sl].astype(bf), old.astype(bf), preferred_element_type=f32)
            outer = lax.dot_general(
                k_s[rows, sl].astype(bf), v_s[rows, sl].astype(bf), (((0,), (0,)), ((), ())),
                preferred_element_type=f32,
            )
            stage[b, h] = dec_s[rows, :][0:1, h:h + 1] * old + outer
        store(b).start()

    counts = jnp.broadcast_to(cvec_ref[...].astype(f32), (8, batch))
    row = lax.broadcasted_iota(jnp.int32, (own, batch), 0)
    seq = lax.broadcasted_iota(jnp.int32, (own, batch), 1)
    count_col = jnp.sum(jnp.where((row // steps) == seq, counts[0:1, :], 0.0), axis=1, keepdims=True)
    live = (lax.broadcasted_iota(jnp.int32, (own, 1), 0) % steps).astype(f32) < count_col
    for h in range(heads):
        sl = slice(h * dim, (h + 1) * dim)
        num = num_s[:, sl] + cs_s[:, h:h + 1] * car_s[:, sl]
        centered = num - jnp.mean(num, axis=1, keepdims=True)
        normal = centered * lax.rsqrt(jnp.mean(centered * centered, axis=1, keepdims=True) + epsilon)
        gate = gt_ref[:, sl].astype(f32)
        mixed = normal * og_ref[layer, h:h + 1, :] + sg_ref[layer:layer + 1, sl] * conv_s[:, sl].astype(f32)
        mixed = mixed * (gate * jax.nn.sigmoid(gate))
        mixed_ref[:, sl] = jnp.where(live, mixed, 0.0).astype(bf)
    for b in range(batch):
        store(b).wait()


def memory_cell(layer, steps, counts, bias_input, bias_forget, branch, gate, old_max, state, conv_weight,
                w_input_gate, w_forget_gate, out_gain, skip_gain, w_query, w_key, w_value, memory, previous):
    layers, batch, heads, dim, _ = memory.shape
    own, width = branch.shape
    f32 = jnp.float32
    smem = pl.BlockSpec(memory_space=pltpu.SMEM)
    anyspace = pl.BlockSpec(memory_space=pl.ANY)
    args = [counts, bias_input, bias_forget, counts[None, :], branch, gate, old_max, state, conv_weight,
            w_input_gate, w_forget_gate, out_gain, skip_gain, w_query, w_key, w_value, memory]
    specs = [smem] * 3 + [VM] * 10 + [anyspace] * 4
    aliases = {}
    if previous is not None:
        aliases = {len(args): 2}
        args += list(previous)
        specs += [anyspace, VM, VM]
    big = pltpu.VMEM((own, width), f32)
    small = pltpu.VMEM((own, 128), f32)
    return pl.pallas_call(
        functools.partial(cell_kernel, layer, heads, steps),
        out_shape=(
            jax.ShapeDtypeStruct((own, width), jnp.bfloat16),
            jax.ShapeDtypeStruct((layers, CONV - 1, batch, width), jnp.bfloat16),
            jax.ShapeDtypeStruct(memory.shape, f32),
            jax.ShapeDtypeStruct((layers, heads, batch), f32),
        ),
        in_specs=specs,
        out_specs=(VM, VM, anyspace, VM),
        scratch_shapes=[
            pltpu.VMEM((batch, 8 + steps, width), f32),
            pltpu.VMEM((own, width), jnp.bfloat16),
            big, big, big, big, big, small, small,
            pltpu.VMEM((CONV - 1, batch, width), f32),
            pltpu.VMEM((3, heads, dim, dim), jnp.bfloat16),
            pltpu.VMEM((batch, heads, dim, dim), f32),
            pltpu.SemaphoreType.DMA((batch,)), pltpu.SemaphoreType.DMA((batch,)),
            pltpu.SemaphoreType.DMA((3,)),
        ],
        input_output_aliases=aliases,
        compiler_params=pltpu.CompilerParams(vmem_limit_bytes=FULL_VMEM),
        name="memory_cell",
    )(*args)


def per_device(tokens, live_counts, norm_gain, w_branch, w_silu_gate, conv_weight, w_query, w_key,
               w_value, w_input_gate, w_forget_gate, bias_input, bias_forget, out_gain, skip_gain,
               w_out, conv_state, memory, max_state):
    ndp = lax.axis_size("dp")
    ntp = lax.axis_size("tp")
    steps, features = tokens.shape[1:]
    own = live_counts.shape[0] * steps
    lanes = -(-own // 128) * 128
    chunks = 4 if own % 64 == 0 else 1
    stream = tokens.reshape(ndp, chunks, own // chunks, features)
    old_max = jnp.transpose(max_state, (0, 2, 1))
    states = jnp.transpose(conv_state, (0, 2, 1, 3))
    link = functools.partial(bridge, ndp, ntp, lanes)
    inputs = dict(gain=norm_gain, w_branch=w_branch, w_gate=w_silu_gate)

    branch, gate = link("enter", 0, FULL_VMEM, stream, li=0, **inputs)
    previous = None
    for l in range(LAYERS):
        mixed, new_conv, new_memory, new_max = memory_cell(
            l, steps, live_counts, bias_input, bias_forget, branch, gate, old_max, states, conv_weight,
            w_input_gate, w_forget_gate, out_gain, skip_gain, w_query, w_key, w_value, memory, previous
        )
        previous = (new_memory, new_conv, new_max)
        if l + 1 < LAYERS:
            stream, branch, gate = link(
                f"bridge{l}", l + 1, FULL_VMEM, stream, lo=l, li=l + 1, mixed=mixed, w_out=w_out, **inputs
            )
        else:
            (stream,) = link("leave", l + 1, LEAVE_VMEM, stream, lo=l, mixed=mixed, w_out=w_out)
    return (stream.reshape(tokens.shape), jnp.transpose(new_conv, (0, 2, 1, 3)), new_memory,
            jnp.transpose(new_max, (0, 2, 1)))


def solution(mesh):
    in_specs = (
        P("grp", None, "dp"),
        P(("grp", "dp")),
        P(None, "dp"),
        P(None, "dp", "tp"),
        P(None, "dp", "tp"),
        P(None, None, "tp"),
        P(None, "tp", None, None),
        P(None, "tp", None, None),
        P(None, "tp", None, None),
        P(None, "tp", None),
        P(None, "tp", None),
        P(None, "tp"),
        P(None, "tp"),
        P(None, "tp", None),
        P(None, "tp"),
        P(None, "tp", "dp"),
        P(None, ("grp", "dp"), None, "tp"),
        P(None, ("grp", "dp"), "tp", None, None),
        P(None, ("grp", "dp"), "tp"),
    )
    out_specs = (
        P("grp", None, "dp"),
        P(None, ("grp", "dp"), None, "tp"),
        P(None, ("grp", "dp"), "tp", None, None),
        P(None, ("grp", "dp"), "tp"),
    )
    return jax.shard_map(
        per_device, mesh=mesh, in_specs=in_specs, out_specs=out_specs, check_vma=False
    )
```

```python
import functools

import jax
import jax.numpy as jnp
from jax import lax
from jax.experimental import pallas as pl
from jax.experimental.pallas import tpu as pltpu
from jax.sharding import PartitionSpec as P

HEAD_DIM = 256
CONV = 4
LAYERS = 2
epsilon = 1e-06
very_negative = -1e30

FULL_VMEM = 60 * 1024 * 1024
LEAVE_VMEM = 24 * 1024 * 1024

VM = pl.BlockSpec(memory_space=pltpu.VMEM)
MESH = pl.DeviceIdType.MESH


def rcopy(src, dst, send, recv, axis, device):
    return pltpu.make_async_remote_copy(
        src_ref=src, dst_ref=dst, send_sem=send, recv_sem=recv,
        device_id={axis: device}, device_id_type=MESH,
    )


def bridge_kernel(ndp, ntp, do_out, do_in, lo, li, names, *refs):
    R = dict(zip(names, refs))
    f32 = jnp.float32
    bf = jnp.bfloat16
    nx = ndp // 2
    me = lax.axis_index("dp")
    core = me % 2
    x = me // 2
    partner = me + 1 - 2 * core
    z = lax.axis_index("tp")
    tok = R["tok_s"]
    chunks, piece, feats = tok.shape[1:]
    own = chunks * piece
    halves = 2 if chunks > 1 else 1
    step = chunks // halves
    pieces = {}
    for h in range(halves):
        pieces[h] = list(range(h * step, (h + 1) * step))

    def load(name, layer):
        return pltpu.make_async_copy(R[name].at[layer], R[name + "_s"], R[name + "_m"])

    def bring(name):
        return pltpu.make_async_copy(R[name], R[name + "_s"], R[name + "_m"])

    for name in ("m", "tok") if do_out else ("tok", "gain"):
        bring(name).start()
    wanted = ([("wo", lo)] if do_out else []) + ([("wb", li), ("wg", li)] if do_in else [])
    for name, layer in wanted:
        load(name, layer).start()
    if do_out and do_in:
        bring("gain").start()
    barrier = pltpu.get_barrier_semaphore()
    for off in range(1, ndp):
        pl.semaphore_signal(barrier, inc=1, device_id={"dp": (me + off) % ndp}, device_id_type=MESH)
    greeted = ndp - 1
    if do_out and ntp > 1:
        @pl.when(z > 0)
        def _():
            pl.semaphore_signal(barrier, inc=1, device_id={"tp": z - 1}, device_id_type=MESH)

        @pl.when(z < ntp - 1)
        def _():
            pl.semaphore_signal(barrier, inc=1, device_id={"tp": z + 1}, device_id_type=MESH)
        greeted = greeted + jnp.where(z > 0, 1, 0) + jnp.where(z < ntp - 1, 1, 0)
    if do_out:
        bring("m").wait()
    pl.semaphore_wait(barrier, greeted)

    def ahead(g):
        return (x + 1 + g) % nx

    def behind(g):
        return (x + nx - 1 - g) % nx

    groups = [("mine", nx - 1, h) for h in range(halves)]
    groups += [("other", nx - 1, 0)]
    for g in range(nx - 1):
        for h in range(halves):
            groups += [("mine", g, h), ("other", g, h)]
    groups += [("other", nx - 1, h) for h in range(1, halves)]
    if not do_out:
        groups = [(kind, g, h) for g in range(nx) for h in range(halves) for kind in ("other", "mine")]

    if do_out:
        m_ref, got, psum = R["m_s"], R["got"], R["psum"]
        width = m_ref.shape[2]
        fresh = R["fresh"]

        def device(kind, g):
            if g == nx - 1:
                return me if kind == "mine" else partner
            return 2 * behind(g) + (core if kind == "mine" else 1 - core)

        def across(g, c):
            return rcopy(m_ref.at[c], got.at[x, core, c], R["ga_s"].at[g, c], R["ga_r"].at[g, c],
                         "dp", 2 * ahead(g) + core)

        def near(c):
            return rcopy(m_ref.at[c], got.at[x, core, c], R["gp_s"].at[c], R["gp_r"].at[c],
                         "dp", partner)

        def passed(g, c):
            spot = got.at[behind(g), core, c]
            return rcopy(spot, spot, R["gf_s"].at[g, c], R["gf_r"].at[g, c], "dp", partner)

        for c in range(chunks):
            for g in range(nx - 1):
                across(g, c).start()
        for c in range(chunks):
            near(c).start()
        load("wo", lo).wait()
        bring("tok").wait()

        def rows_of(kind, g, h):
            if g == nx - 1:
                if kind == "mine":
                    return m_ref[h * step:(h + 1) * step]
                for c in pieces[h]:
                    near(c).wait_recv()
                return got[x, 1 - core, h * step:(h + 1) * step]
            if kind == "mine":
                for c in pieces[h]:
                    across(g, c).wait_recv()
                    passed(g, c).start()
                return got[behind(g), core, h * step:(h + 1) * step]
            for c in pieces[h]:
                passed(g, c).wait_recv()
            return got[behind(g), 1 - core, h * step:(h + 1) * step]

        def product_out(i):
            rows = rows_of(*groups[i]).reshape(step * piece, width)
            part = jnp.dot(rows, R["wo_s"][...], preferred_element_type=f32)
            psum[i * step:(i + 1) * step] = part.reshape(step, piece, feats)

        half = ntp // 2
        zsum, zin, zcross = R["zsum"], R["zin"], R["zcross"]
        left = z < half
        inward = jnp.where(left, z + 1, z - 1)
        outward = jnp.where(left, z - 1, z + 1)
        edge = (z == 0) | (z == ntp - 1)
        center = (z == half - 1) | (z == half)
        inner = jnp.logical_not(edge)
        outer = jnp.logical_not(center)
        spots = len(groups) * step

        def spot_of(p):
            kind, g, h = groups[p // step]
            return device(kind, g), h * step + p % step

        def up(p):
            return rcopy(zsum.at[p], zin.at[p], R["zi_s"].at[p], R["zi_r"].at[p], "tp", inward)

        def cross(p):
            return rcopy(zsum.at[p], zcross.at[p], R["zc_s"].at[p], R["zc_r"].at[p], "tp", inward)

        def down(p):
            d, c = spot_of(p)
            return rcopy(fresh.at[d, c], fresh.at[d, c], R["zo_s"].at[p], R["zo_r"].at[p], "tp", outward)

        def settle(p, total):
            d, c = spot_of(p)
            update = total.astype(bf).astype(f32)
            fresh[d, c] = (tok[d, c].astype(f32) + update).astype(bf)

        def gathered(p):
            up(p).wait_recv()
            return psum[p] + zin[p].astype(f32)

    if do_in:
        ob, og, oaux, aux_s = R["ob"], R["og"], R["oaux"], R["aux_s"]
        snd, loc, r1, s2, r2 = R["snd"], R["loc"], R["r1"], R["s2"], R["r2"]
        wide = snd.shape[-1]
        weights = (R["wb_s"], R["wg_s"])
        source = fresh if do_out else tok
        aux_s[...] = jnp.zeros_like(aux_s)

        def target(kind, g):
            if g == nx - 1:
                return me if kind == "mine" else partner
            return 2 * ahead(g) + (core if kind == "mine" else 1 - core)

        def first(g, k, c):
            return rcopy(snd.at[g, k, c], r1.at[g, k, c], R["r1_s"].at[g, k, c], R["r1_r"].at[g, k, c],
                         "dp", partner)

        def second(g, k, c):
            return rcopy(s2.at[g, k, c], r2.at[g, k, c], R["r2_s"].at[g, k, c], R["r2_r"].at[g, k, c],
                         "dp", 2 * ahead(g) + core)

        def tell(kind, g):
            d = target(kind, g)
            i = 0 if kind == "mine" else 1
            return rcopy(aux_s.at[d], oaux.at[me], R["ax_s"].at[g, i], R["ax_r"].at[g, i], "dp", d)

        def forward(g, h):
            for k in range(2):
                for c in pieces[h]:
                    first(g, k, c).wait_recv()
                    s2[g, k, c] = (loc[g, k, c].astype(f32) + r1[g, k, c].astype(f32)).astype(bf)
                    second(g, k, c).start()

        def handle(kind, g, h, done, waiting):
            gw = g
            if do_out and g < nx - 1:
                gw = nx - 2 - g
            d = target(kind, gw)
            size = step * piece
            rows = source[d, h * step:(h + 1) * step].reshape(size, feats).astype(f32)
            square = jnp.sum(rows * rows, axis=1, keepdims=True)
            r = lax.broadcasted_iota(jnp.int32, (size, own), 0) + h * size
            c = lax.broadcasted_iota(jnp.int32, (size, own), 1)
            line = jnp.sum(jnp.where(r == c, square, 0.0), axis=0, keepdims=True)
            if h == 0:
                aux_s[d, 0:1, :own] = line
            else:
                aux_s[d, 0:1, :own] += line
            done.append((kind, gw))
            scaled = (rows * R["gain_s"][li:li + 1, :]).astype(bf)
            for k in range(2):
                part = jnp.dot(scaled, weights[k][...], preferred_element_type=f32).astype(bf)
                part = part.reshape(step, piece, wide)
                if kind == "mine":
                    loc[gw, k, h * step:(h + 1) * step] = part
                else:
                    snd[gw, k, h * step:(h + 1) * step] = part
                    for c in pieces[h]:
                        first(gw, k, c).start()
            if done.count((kind, gw)) == halves:
                if (kind, gw) == ("mine", nx - 1):
                    oaux[me] = aux_s[me]
                else:
                    tell(kind, gw).start()
            while waiting:
                forward(*waiting.pop(0))
            if gw < nx - 1:
                pair = [(a, gw, h) for a in ("mine", "other")]
                done.append(("seen", kind, gw, h))
                if all(("seen",) + a in done for a in pair):
                    waiting.append((gw, h))

        def flush(waiting):
            while waiting:
                forward(*waiting.pop(0))

    if do_in:
        bring("gain").wait()
        if not do_out:
            bring("tok").wait()
        for name in ("wb", "wg"):
            load(name, li).wait()
    if not do_out:
        done, waiting = [], []
        for group in groups:
            handle(*group, done, waiting)
        flush(waiting)
    else:
        def finish(i, done, waiting):
            if do_in:
                handle(*groups[i], done, waiting)

        if ntp == 1:
            done, waiting = [], []
            for i in range(len(groups)):
                product_out(i)
                for p in range(i * step, (i + 1) * step):
                    settle(p, psum[p])
                finish(i, done, waiting)
            if do_in:
                flush(waiting)
        else:
            if ntp > 2:
                @pl.when(outer)
                def _():
                    done, waiting = [], []
                    for i in range(len(groups)):
                        product_out(i)
                        for p in range(i * step, (i + 1) * step):
                            if ntp == 4:
                                zsum[p] = psum[p].astype(bf)
                            else:
                                @pl.when(edge)
                                def _():
                                    zsum[p] = psum[p].astype(bf)

                                @pl.when(inner)
                                def _():
                                    zsum[p] = gathered(p).astype(bf)
                            up(p).start()
                    for i in range(len(groups)):
                        for p in range(i * step, (i + 1) * step):
                            down(p).wait_recv()
                            if ntp > 4:
                                @pl.when(inner)
                                def _():
                                    down(p).start()
                        finish(i, done, waiting)
                    if do_in:
                        flush(waiting)
                    for p in range(spots):
                        up(p).wait_send()
                        if ntp > 4:
                            @pl.when(inner)
                            def _():
                                down(p).wait_send()

            @pl.when(center)
            def _():
                done, waiting = [], []
                lag = 4
                for p in range(spots + lag):
                    if p < spots:
                        if p % step == 0:
                            product_out(p // step)
                        zsum[p] = (gathered(p) if ntp > 2 else psum[p]).astype(bf)
                        cross(p).start()
                    q = p - lag
                    if q >= 0:
                        cross(q).wait_recv()
                        settle(q, zsum[q].astype(f32) + zcross[q].astype(f32))
                        if ntp > 2:
                            down(q).start()
                        if q % step == step - 1:
                            finish(q // step, done, waiting)
                if do_in:
                    flush(waiting)
                for p in range(spots):
                    cross(p).wait_send()
                    if ntp > 2:
                        down(p).wait_send()

        for c in range(chunks):
            near(c).wait_send()
            for g in range(nx - 1):
                across(g, c).wait_send()
                passed(g, c).wait_send()

    if do_out and do_in:
        keep = pltpu.make_async_copy(fresh, R["fresh_o"], R["fresh_m"])
        keep.start()
    if do_in:
        last = nx - 1
        for g in range(nx):
            for i, kind in enumerate(("mine", "other")):
                if (kind, g) != ("mine", last):
                    tell(kind, g).wait_recv()
        total = oaux[0, 0:1, :own]
        for d in range(1, ndp):
            total = total + oaux[d, 0:1, :own]
        inv_row = lax.rsqrt(total / (feats * ndp) + epsilon)
        r = lax.broadcasted_iota(jnp.int32, (own, own), 0)
        c = lax.broadcasted_iota(jnp.int32, (own, own), 1)
        inv = jnp.sum(jnp.where(r == c, inv_row, 0.0), axis=1, keepdims=True)
        for h in range(halves):
            for k, out in ((0, ob), (1, og)):
                for c in pieces[h]:
                    first(last, k, c).wait_recv()
                    total = loc[last, k, c].astype(f32) + r1[last, k, c].astype(f32)
                    for g in range(nx - 1):
                        second(g, k, c).wait_recv()
                        total = total + r2[g, k, c].astype(f32)
                    out[c * piece:(c + 1) * piece, :] = (
                        total * inv[c * piece:(c + 1) * piece, :]
                    ).astype(bf)
        if do_out:
            keep.wait()
        for g in range(nx):
            for kind in ("mine", "other"):
                if (kind, g) != ("mine", last):
                    tell(kind, g).wait_send()
            for k in range(2):
                for c in range(chunks):
                    first(g, k, c).wait_send()
                    if g < last:
                        second(g, k, c).wait_send()


def bridge(ndp, ntp, lanes, name, cid, limit, tok, lo=None, li=None, mixed=None, w_out=None, gain=None,
           w_branch=None, w_gate=None):
    f32 = jnp.float32
    bf = jnp.bfloat16
    do_out = mixed is not None
    do_in = w_branch is not None
    nx = ndp // 2
    far = max(nx - 1, 1)
    chunks, piece, feats = tok.shape[1:]
    own = chunks * piece
    spots = ndp * chunks
    weight = pl.BlockSpec(memory_space=pl.ANY)
    sem = pltpu.SemaphoreType.DMA
    names, args, specs, outs, scratch = [], [], [], [], []

    def take(key, a, spec=VM):
        names.append(key)
        args.append(a)
        specs.append(spec)

    take("tok", tok, weight)
    if do_out:
        width = mixed.shape[-1]
        take("m", mixed.reshape(chunks, piece, width), weight)
        take("wo", w_out, weight)
    if do_in:
        width = w_branch.shape[-1]
        take("gain", gain, weight)
        take("wb", w_branch, weight)
        take("wg", w_gate, weight)

    def give(key, shape, dtype):
        names.append(key)
        outs.append(jax.ShapeDtypeStruct(shape, dtype))

    if do_out:
        give("fresh_o" if do_in else "fresh", tok.shape, bf)
    if do_in:
        give("ob", (own, width), bf)
        give("og", (own, width), bf)

    def room(key, shape, dtype):
        names.append(key)
        scratch.append(pltpu.VMEM(shape, dtype))

    def flag(key, *shape):
        names.append(key)
        scratch.append(sem(shape) if shape else sem)

    def sems(key, *shape):
        flag(key + "_s", *shape)
        flag(key + "_r", *shape)

    room("tok_s", tok.shape, bf)
    flag("tok_m")
    if do_in:
        room("gain_s", gain.shape, f32)
        flag("gain_m")
    if do_out:
        room("m_s", (chunks, piece, width), bf)
        flag("m_m")
        if do_in:
            room("fresh", tok.shape, bf)
            flag("fresh_m")
        room("got", (nx, 2, chunks, piece, width), bf)
        room("psum", (spots, piece, feats), f32)
        room("wo_s", w_out.shape[1:], bf)
        flag("wo_m")
        for key in ("zsum", "zin", "zcross"):
            room(key, (spots, piece, feats), bf)
        sems("ga", far, chunks)
        sems("gf", far, chunks)
        sems("gp", chunks)
        for key in ("zi", "zc", "zo"):
            sems(key, spots)
    if do_in:
        for key, a in (("wb", w_branch), ("wg", w_gate)):
            room(key + "_s", a.shape[1:], bf)
            flag(key + "_m")
        room("aux_s", (ndp, 8, lanes), f32)
        room("oaux", (ndp, 8, lanes), f32)
        for key, count in (("snd", nx), ("loc", nx), ("r1", nx), ("s2", far), ("r2", far)):
            room(key, (count, 2, chunks, piece, width), bf)
        sems("r1", nx, 2, chunks)
        sems("r2", far, 2, chunks)
        sems("ax", nx, 2)
    return pl.pallas_call(
        functools.partial(bridge_kernel, ndp, ntp, do_out, do_in, lo, li, names),
        out_shape=tuple(outs),
        in_specs=specs,
        out_specs=((weight, VM, VM) if do_out and do_in else (VM,) * len(outs)),
        scratch_shapes=scratch,
        compiler_params=pltpu.CompilerParams(
            collective_id=cid, has_side_effects=True, vmem_limit_bytes=limit
        ),
        name=name,
    )(*args)


def cell_kernel(layer, heads, steps, cnt_any, cvec_any, br_any, gt_any, mrow_any, bi_any, bf_any, st_any,
                cw_any, wi_any, wf_any, og_any, sg_any, wq_ref, wk_ref, wv_ref, mem_ref, *rest):
    (mixed_any, nc_any, newmem_ref, nmax_any,
     cnt_ref, cvec_ref, br_ref, gt_ref, mrow_ref, bi_ref, bf_ref, st_ref, cw_ref, wi_ref, wf_ref, og_ref,
     sg_ref, mixed_ref, nc_ref, nmax_ref,
     pad_s, conv_s, q_s, k_s, v_s, num_s, car_s, dec_s, cs_s, nc_s, w_s, stage, ins, outs,
     w_sem, s_sem, o_sem) = rest[-37:]
    f32 = jnp.float32
    bf = jnp.bfloat16
    batch = stage.shape[0]
    own, width = br_ref.shape
    dim = HEAD_DIM
    base = 8 - (CONV - 1)

    def fetch(b):
        return pltpu.make_async_copy(mem_ref.at[layer, b], stage.at[b], ins.at[b])

    def store(b):
        return pltpu.make_async_copy(stage.at[b], newmem_ref.at[layer, b], outs.at[b])

    maps = [
        pltpu.make_async_copy(w_ref.at[layer], w_s.at[i], w_sem.at[i])
        for i, w_ref in enumerate((wq_ref, wk_ref, wv_ref))
    ]
    smalls = [
        pltpu.make_async_copy(a, b, s_sem.at[i])
        for i, (a, b) in enumerate((
            (br_any, br_ref), (st_any.at[layer], st_ref), (cw_any, cw_ref), (cnt_any, cnt_ref),
            (cvec_any, cvec_ref), (mrow_any, mrow_ref), (bi_any, bi_ref), (bf_any, bf_ref),
            (wi_any, wi_ref), (wf_any, wf_ref), (og_any, og_ref), (sg_any, sg_ref), (gt_any, gt_ref),
        ))
    ]
    for cp in smalls[:8]:
        cp.start()
    for cp in maps:
        cp.start()
    for cp in smalls[8:]:
        cp.start()

    @pl.loop(0, batch)
    def _(b):
        fetch(b).start()
    for cp in smalls:
        cp.wait()

    r = lax.broadcasted_iota(jnp.int32, (own, own), 0)
    c = lax.broadcasted_iota(jnp.int32, (own, own), 1)
    row = lax.broadcasted_iota(jnp.int32, (own, batch), 0)
    seq = lax.broadcasted_iota(jnp.int32, (own, batch), 1)
    belongs = (row // steps) == seq
    closing = row == seq * steps + (steps - 1)
    nt = (((1,), (1,)), ((), ()))
    spread = jnp.where(belongs, 1.0, 0.0)
    counts = jnp.broadcast_to(cvec_ref[...].astype(f32), (8, batch))
    count_row = lax.dot_general(counts, spread, nt, preferred_element_type=f32)[0:1, :]
    count_col = jnp.sum(jnp.where(belongs, counts[0:1, :], 0.0), axis=1, keepdims=True)
    branch = br_ref[...]
    pad_s[:, 8:8 + steps, :] = branch.astype(f32).reshape(batch, steps, width)
    for j in range(CONV - 1):
        rows = st_ref[j].astype(f32)
        for b in range(batch):
            pad_s[b, base + j:base + j + 1, :] = rows[b:b + 1, :]
    total = pad_s[:, base:base + steps, :] * cw_ref[layer, 0:1, :]
    for j in range(1, CONV):
        total = total + pad_s[:, base + j:base + j + steps, :] * cw_ref[layer, j:j + 1, :]
    conv = (total * jax.nn.sigmoid(total)).astype(bf).reshape(own, width)
    conv_s[...] = conv
    for b in range(batch):
        for i in range(CONV - 1):
            nc_s[i, b:b + 1, :] = pad_s[b, pl.ds(base + i + cnt_ref[b], 1), :]
    nc_ref[...] = nc_s[...].astype(bf)

    same = (r // steps) == (c // steps)
    causal = same & (r >= c)
    behind = same & (r <= c)
    live_col = (r[:, 0:1] % steps).astype(f32) < count_col
    live_row = (c[0:1, :] % steps).astype(f32) < count_row
    for cp in maps:
        cp.wait()
    def log_sig(x):
        return jnp.minimum(x, 0.0) - jnp.log1p(jnp.exp(-jnp.abs(x)))

    def side(columns):
        lane = lax.broadcasted_iota(jnp.int32, (own, heads), 1)
        out = jnp.broadcast_to(columns[0], (own, heads))
        for h in range(1, heads):
            out = jnp.where(lane == h, columns[h], out)
        return out

    def pile(lines):
        level = lax.broadcasted_iota(jnp.int32, (heads, own), 0)
        out = jnp.broadcast_to(lines[0], (heads, own))
        for h in range(1, heads):
            out = jnp.where(level == h, lines[h], out)
        return out

    exact = lax.Precision.HIGHEST
    cols = ([], [])
    lines = ([], [])
    for h in range(heads):
        sl = slice(h * dim, (h + 1) * dim)
        q = jnp.dot(conv[:, sl], w_s[0, h], preferred_element_type=f32).astype(bf)
        k = jnp.dot(conv[:, sl], w_s[1, h], preferred_element_type=f32).astype(bf)
        v = jnp.dot(branch[:, sl], w_s[2, h], preferred_element_type=f32).astype(bf)
        q_s[:, sl] = q.astype(f32)
        k_s[:, sl] = k.astype(f32) * (dim ** -0.5)
        v_s[:, sl] = v.astype(f32)
        for n, g_ref in enumerate((wi_ref, wf_ref)):
            col = None
            for i, part in enumerate((q, k, v)):
                w = g_ref[layer, :, i * dim:(i + 1) * dim]
                if heads == 1:
                    w = jnp.broadcast_to(w.astype(f32), (8, dim)).astype(bf)
                one = lax.dot_general(part, w, nt, preferred_element_type=f32)
                two = lax.dot_general(w, part, nt, preferred_element_type=f32)
                col, line = (one, two) if col is None else (col + one, line + two)
            cols[n].append(col[:, h:h + 1])
            lines[n].append(line[h:h + 1, :])
    bias_col = [ref[layer:layer + 1, :] for ref in (bi_ref, bf_ref)]
    head_eye = (
        lax.broadcasted_iota(jnp.int32, (heads, heads), 0) == lax.broadcasted_iota(jnp.int32, (heads, heads), 1)
    )
    bias_row = [jnp.sum(jnp.where(head_eye, b, 0.0), axis=1, keepdims=True) for b in bias_col]
    ig_col = jnp.where(live_col, side(cols[0]) + bias_col[0], very_negative)
    fg_col = jnp.where(live_col, log_sig(side(cols[1]) + bias_col[1]), 0.0)
    ig_row = jnp.where(live_row, pile(lines[0]) + bias_row[0], very_negative)
    fg_row = jnp.where(live_row, log_sig(pile(lines[1]) + bias_row[1]), 0.0)
    ones = jnp.where(causal, 1.0, 0.0)
    sames = jnp.where(same, 1.0, 0.0)
    if heads == 1:
        cum_col = jnp.sum(jnp.where(causal, fg_row, 0.0), axis=1, keepdims=True)
        end_col = jnp.sum(jnp.where(same, fg_row, 0.0), axis=1, keepdims=True)
        cum_row = jnp.sum(jnp.where(behind, fg_col, 0.0), axis=0, keepdims=True)
        old_max = jnp.sum(jnp.where(belongs, mrow_ref[layer], 0.0), axis=1, keepdims=True)
    else:
        cum_col = jnp.dot(ones, fg_col, preferred_element_type=f32, precision=exact)
        end_col = jnp.dot(sames, fg_col, preferred_element_type=f32, precision=exact)
        cum_row = lax.dot_general(fg_row, ones, nt, preferred_element_type=f32, precision=exact)
        old_max = lax.dot_general(spread, mrow_ref[layer], nt, preferred_element_type=f32, precision=exact)
    lift_row = ig_row - cum_row
    carried = cum_col + old_max
    tops = []
    ends_ = []
    for h in range(heads):
        lift = lift_row[h:h + 1, :]
        logw = jnp.where(causal, cum_col[:, h:h + 1] + lift, very_negative)
        tops.append(jnp.max(logw, axis=1, keepdims=True))
        ends_.append(jnp.max(jnp.where(same, lift, very_negative), axis=1, keepdims=True))
    stab = jnp.maximum(side(tops), carried)
    new_max = jnp.maximum(end_col + side(ends_), end_col + old_max)
    update = jnp.exp(end_col - cum_col + ig_col - new_max)
    dec_s[:, :heads] = jnp.exp(end_col + old_max - new_max)
    cs_s[:, :heads] = jnp.exp(carried - stab)
    for h in range(heads):
        sl = slice(h * dim, (h + 1) * dim)
        logw = jnp.where(causal, cum_col[:, h:h + 1] + lift_row[h:h + 1, :], very_negative)
        weights = jnp.exp(logw - stab[:, h:h + 1])
        nmax_ref[h:h + 1, :] = jnp.sum(jnp.where(closing, new_max[:, h:h + 1], 0.0), axis=0, keepdims=True)
        scores = lax.dot_general(q_s[:, sl].astype(bf), k_s[:, sl].astype(bf), nt, preferred_element_type=f32)
        scores = (jnp.where(causal, scores, 0.0) * weights).astype(bf)
        num_s[:, sl] = jnp.dot(scores, v_s[:, sl].astype(bf), preferred_element_type=f32)
        k_s[:, sl] = k_s[:, sl] * update[:, h:h + 1]

    def advance(b):
        fetch(b).wait()
        rows = pl.ds(pl.multiple_of(b * steps, 8), steps)
        for h in range(heads):
            sl = slice(h * dim, (h + 1) * dim)
            old = stage[b, h]
            car_s[rows, sl] = jnp.dot(q_s[rows, sl].astype(bf), old.astype(bf), preferred_element_type=f32)
            outer = lax.dot_general(
                k_s[rows, sl].astype(bf), v_s[rows, sl].astype(bf), (((0,), (0,)), ((), ())),
                preferred_element_type=f32,
            )
            stage[b, h] = dec_s[rows, :][0:1, h:h + 1] * old + outer
        store(b).start()

    stride = 2 if batch % 2 == 0 else 1

    @pl.loop(0, batch, step=stride)
    def _(b):
        for i in range(stride):
            advance(b + i)

    counts = jnp.broadcast_to(cvec_ref[...].astype(f32), (8, batch))
    row = lax.broadcasted_iota(jnp.int32, (own, batch), 0)
    seq = lax.broadcasted_iota(jnp.int32, (own, batch), 1)
    count_col = jnp.sum(jnp.where((row // steps) == seq, counts[0:1, :], 0.0), axis=1, keepdims=True)
    live = (lax.broadcasted_iota(jnp.int32, (own, 1), 0) % steps).astype(f32) < count_col
    for h in range(heads):
        sl = slice(h * dim, (h + 1) * dim)
        num = num_s[:, sl] + cs_s[:, h:h + 1] * car_s[:, sl]
        centered = num - jnp.mean(num, axis=1, keepdims=True)
        normal = centered * lax.rsqrt(jnp.mean(centered * centered, axis=1, keepdims=True) + epsilon)
        gate = gt_ref[:, sl].astype(f32)
        mixed = normal * og_ref[layer, h:h + 1, :] + sg_ref[layer:layer + 1, sl] * conv_s[:, sl].astype(f32)
        mixed = mixed * (gate * jax.nn.sigmoid(gate))
        mixed_ref[:, sl] = jnp.where(live, mixed, 0.0).astype(bf)
    ends = [
        pltpu.make_async_copy(a, b, o_sem.at[i])
        for i, (a, b) in enumerate((
            (mixed_ref, mixed_any), (nc_ref, nc_any.at[layer]), (nmax_ref, nmax_any.at[layer])
        ))
    ]
    for cp in ends:
        cp.start()
    for b in range(batch):
        store(b).wait()
    for cp in ends:
        cp.wait()


def memory_cell(layer, steps, counts, bias_input, bias_forget, branch, gate, old_max, state, conv_weight,
                w_input_gate, w_forget_gate, out_gain, skip_gain, w_query, w_key, w_value, memory, previous):
    layers, batch, heads, dim, _ = memory.shape
    own, width = branch.shape
    f32 = jnp.float32
    bf = jnp.bfloat16
    anyspace = pl.BlockSpec(memory_space=pl.ANY)
    args = [counts, counts[None, :], branch, gate, old_max, bias_input, bias_forget, state, conv_weight,
            w_input_gate, w_forget_gate, out_gain, skip_gain, w_query, w_key, w_value, memory]
    held = [pltpu.SMEM(counts.shape, jnp.int32)]
    held += [pltpu.VMEM(a.shape[1:] if a is state else a.shape, a.dtype) for a in args[1:13]]
    held += [
        pltpu.VMEM((own, width), bf),
        pltpu.VMEM((CONV - 1, batch, width), bf),
        pltpu.VMEM((heads, batch), f32),
    ]
    aliases = {}
    if previous is not None:
        aliases = {len(args): 2, len(args) + 1: 1, len(args) + 2: 3}
        args += list(previous)
    specs = [anyspace] * len(args)
    big = pltpu.VMEM((own, width), f32)
    small = pltpu.VMEM((own, 128), f32)
    return pl.pallas_call(
        functools.partial(cell_kernel, layer, heads, steps),
        out_shape=(
            jax.ShapeDtypeStruct((own, width), jnp.bfloat16),
            jax.ShapeDtypeStruct((layers, CONV - 1, batch, width), jnp.bfloat16),
            jax.ShapeDtypeStruct(memory.shape, f32),
            jax.ShapeDtypeStruct((layers, heads, batch), f32),
        ),
        in_specs=specs,
        out_specs=(anyspace,) * 4,
        scratch_shapes=held + [
            pltpu.VMEM((batch, 8 + steps, width), f32),
            pltpu.VMEM((own, width), jnp.bfloat16),
            big, big, big, big, big, small, small,
            pltpu.VMEM((CONV - 1, batch, width), f32),
            pltpu.VMEM((3, heads, dim, dim), jnp.bfloat16),
            pltpu.VMEM((batch, heads, dim, dim), f32),
            pltpu.SemaphoreType.DMA((batch,)), pltpu.SemaphoreType.DMA((batch,)),
            pltpu.SemaphoreType.DMA((3,)), pltpu.SemaphoreType.DMA((13,)), pltpu.SemaphoreType.DMA((3,)),
        ],
        input_output_aliases=aliases,
        compiler_params=pltpu.CompilerParams(vmem_limit_bytes=FULL_VMEM),
        name="memory_cell",
    )(*args)


def per_device(tokens, live_counts, norm_gain, w_branch, w_silu_gate, conv_weight, w_query, w_key,
               w_value, w_input_gate, w_forget_gate, bias_input, bias_forget, out_gain, skip_gain,
               w_out, conv_state, memory, max_state):
    ndp = lax.axis_size("dp")
    ntp = lax.axis_size("tp")
    steps, features = tokens.shape[1:]
    own = live_counts.shape[0] * steps
    lanes = -(-own // 128) * 128
    chunks = 4 if own % 64 == 0 else 1
    stream = tokens.reshape(ndp, chunks, own // chunks, features)
    old_max = jnp.transpose(max_state, (0, 2, 1))
    states = jnp.transpose(conv_state, (0, 2, 1, 3))
    link = functools.partial(bridge, ndp, ntp, lanes)
    inputs = dict(gain=norm_gain, w_branch=w_branch, w_gate=w_silu_gate)

    branch, gate = link("enter", 0, FULL_VMEM, stream, li=0, **inputs)
    previous = None
    for l in range(LAYERS):
        mixed, new_conv, new_memory, new_max = memory_cell(
            l, steps, live_counts, bias_input, bias_forget, branch, gate, old_max, states, conv_weight,
            w_input_gate, w_forget_gate, out_gain, skip_gain, w_query, w_key, w_value, memory, previous
        )
        previous = (new_memory, new_conv, new_max)
        if l + 1 < LAYERS:
            stream, branch, gate = link(
                f"bridge{l}", l + 1, FULL_VMEM, stream, lo=l, li=l + 1, mixed=mixed, w_out=w_out, **inputs
            )
        else:
            (stream,) = link("leave", l + 1, LEAVE_VMEM, stream, lo=l, mixed=mixed, w_out=w_out)
    return (stream.reshape(tokens.shape), jnp.transpose(new_conv, (0, 2, 1, 3)), new_memory,
            jnp.transpose(new_max, (0, 2, 1)))


def solution(mesh):
    in_specs = (
        P("grp", None, "dp"),
        P(("grp", "dp")),
        P(None, "dp"),
        P(None, "dp", "tp"),
        P(None, "dp", "tp"),
        P(None, None, "tp"),
        P(None, "tp", None, None),
        P(None, "tp", None, None),
        P(None, "tp", None, None),
        P(None, "tp", None),
        P(None, "tp", None),
        P(None, "tp"),
        P(None, "tp"),
        P(None, "tp", None),
        P(None, "tp"),
        P(None, "tp", "dp"),
        P(None, ("grp", "dp"), None, "tp"),
        P(None, ("grp", "dp"), "tp", None, None),
        P(None, ("grp", "dp"), "tp"),
    )
    out_specs = (
        P("grp", None, "dp"),
        P(None, ("grp", "dp"), None, "tp"),
        P(None, ("grp", "dp"), "tp", None, None),
        P(None, ("grp", "dp"), "tp"),
    )
    return jax.shard_map(
        per_device, mesh=mesh, in_specs=in_specs, out_specs=out_specs, check_vma=False
    )
```

```python
import functools

import jax
import jax.numpy as jnp
from jax import lax
from jax.experimental import pallas as pl
from jax.experimental.pallas import tpu as pltpu
from jax.sharding import PartitionSpec as P

HEAD_DIM = 256
CONV = 4
LAYERS = 2
epsilon = 1e-06
very_negative = -1e30

FULL_VMEM = 60 * 1024 * 1024
LEAVE_VMEM = 24 * 1024 * 1024

VM = pl.BlockSpec(memory_space=pltpu.VMEM)
MESH = pl.DeviceIdType.MESH


def rcopy(src, dst, send, recv, axis, device):
    return pltpu.make_async_remote_copy(
        src_ref=src, dst_ref=dst, send_sem=send, recv_sem=recv,
        device_id={axis: device}, device_id_type=MESH,
    )


def bridge_kernel(ndp, ntp, do_out, do_in, lo, li, names, *refs):
    R = dict(zip(names, refs))
    f32 = jnp.float32
    bf = jnp.bfloat16
    nx = ndp // 2
    me = lax.axis_index("dp")
    core = me % 2
    x = me // 2
    partner = me + 1 - 2 * core
    z = lax.axis_index("tp")
    tok = R["tok_s"]
    chunks, piece, feats = tok.shape[1:]
    own = chunks * piece
    halves = 2 if chunks > 1 else 1
    step = chunks // halves
    pieces = {}
    for h in range(halves):
        pieces[h] = list(range(h * step, (h + 1) * step))

    def load(name, layer):
        return pltpu.make_async_copy(R[name].at[layer], R[name + "_s"], R[name + "_m"])

    def bring(name):
        return pltpu.make_async_copy(R[name], R[name + "_s"], R[name + "_m"])

    for name in ("m", "tok") if do_out else ("tok", "gain"):
        bring(name).start()
    wanted = ([("wo", lo)] if do_out else []) + ([("wb", li), ("wg", li)] if do_in else [])
    for name, layer in wanted:
        load(name, layer).start()
    if do_out and do_in:
        bring("gain").start()
    barrier = pltpu.get_barrier_semaphore()
    for off in range(1, ndp):
        pl.semaphore_signal(barrier, inc=1, device_id={"dp": (me + off) % ndp}, device_id_type=MESH)
    greeted = ndp - 1
    if do_out and ntp > 1:
        @pl.when(z > 0)
        def _():
            pl.semaphore_signal(barrier, inc=1, device_id={"tp": z - 1}, device_id_type=MESH)

        @pl.when(z < ntp - 1)
        def _():
            pl.semaphore_signal(barrier, inc=1, device_id={"tp": z + 1}, device_id_type=MESH)
        greeted = greeted + jnp.where(z > 0, 1, 0) + jnp.where(z < ntp - 1, 1, 0)
    if do_out:
        bring("m").wait()
    pl.semaphore_wait(barrier, greeted)

    def ahead(g):
        return (x + 1 + g) % nx

    def behind(g):
        return (x + nx - 1 - g) % nx

    groups = [("mine", nx - 1, h) for h in range(halves)]
    groups += [("other", nx - 1, 0)]
    for g in range(nx - 1):
        for h in range(halves):
            groups += [("mine", g, h), ("other", g, h)]
    groups += [("other", nx - 1, h) for h in range(1, halves)]
    if not do_out:
        groups = [(kind, g, h) for g in range(nx) for h in range(halves) for kind in ("other", "mine")]

    if do_out:
        m_ref, got, psum = R["m_s"], R["got"], R["psum"]
        width = m_ref.shape[2]
        fresh = R["fresh"]

        def device(kind, g):
            if g == nx - 1:
                return me if kind == "mine" else partner
            return 2 * behind(g) + (core if kind == "mine" else 1 - core)

        def across(g, c):
            return rcopy(m_ref.at[c], got.at[x, core, c], R["ga_s"].at[g, c], R["ga_r"].at[g, c],
                         "dp", 2 * ahead(g) + core)

        def near(c):
            return rcopy(m_ref.at[c], got.at[x, core, c], R["gp_s"].at[c], R["gp_r"].at[c],
                         "dp", partner)

        def passed(g, c):
            spot = got.at[behind(g), core, c]
            return rcopy(spot, spot, R["gf_s"].at[g, c], R["gf_r"].at[g, c], "dp", partner)

        for c in range(chunks):
            for g in range(nx - 1):
                across(g, c).start()
        for c in range(chunks):
            near(c).start()
        load("wo", lo).wait()
        bring("tok").wait()

        def rows_of(kind, g, h):
            if g == nx - 1:
                if kind == "mine":
                    return m_ref[h * step:(h + 1) * step]
                for c in pieces[h]:
                    near(c).wait_recv()
                return got[x, 1 - core, h * step:(h + 1) * step]
            if kind == "mine":
                for c in pieces[h]:
                    across(g, c).wait_recv()
                    passed(g, c).start()
                return got[behind(g), core, h * step:(h + 1) * step]
            for c in pieces[h]:
                passed(g, c).wait_recv()
            return got[behind(g), 1 - core, h * step:(h + 1) * step]

        def product_out(i):
            rows = rows_of(*groups[i]).reshape(step * piece, width)
            part = jnp.dot(rows, R["wo_s"][...], preferred_element_type=f32)
            psum[i * step:(i + 1) * step] = part.reshape(step, piece, feats)

        half = ntp // 2
        zsum, zin, zcross = R["zsum"], R["zin"], R["zcross"]
        left = z < half
        inward = jnp.where(left, z + 1, z - 1)
        outward = jnp.where(left, z - 1, z + 1)
        edge = (z == 0) | (z == ntp - 1)
        center = (z == half - 1) | (z == half)
        inner = jnp.logical_not(edge)
        outer = jnp.logical_not(center)
        spots = len(groups) * step

        def spot_of(p):
            kind, g, h = groups[p // step]
            return device(kind, g), h * step + p % step

        def up(p):
            return rcopy(zsum.at[p], zin.at[p], R["zi_s"].at[p], R["zi_r"].at[p], "tp", inward)

        def cross(p):
            return rcopy(zsum.at[p], zcross.at[p], R["zc_s"].at[p], R["zc_r"].at[p], "tp", inward)

        def down(p):
            d, c = spot_of(p)
            return rcopy(fresh.at[d, c], fresh.at[d, c], R["zo_s"].at[p], R["zo_r"].at[p], "tp", outward)

        def settle(p, total):
            d, c = spot_of(p)
            update = total.astype(bf).astype(f32)
            fresh[d, c] = (tok[d, c].astype(f32) + update).astype(bf)

        def gathered(p):
            up(p).wait_recv()
            return psum[p] + zin[p].astype(f32)

    if do_in:
        ob, og, oaux, aux_s = R["ob"], R["og"], R["oaux"], R["aux_s"]
        snd, loc, r1, s2, r2 = R["snd"], R["loc"], R["r1"], R["s2"], R["r2"]
        wide = snd.shape[-1]
        weights = (R["wb_s"], R["wg_s"])
        source = fresh if do_out else tok
        aux_s[...] = jnp.zeros_like(aux_s)

        def target(kind, g):
            if g == nx - 1:
                return me if kind == "mine" else partner
            return 2 * ahead(g) + (core if kind == "mine" else 1 - core)

        def first(g, k, c):
            return rcopy(snd.at[g, k, c], r1.at[g, k, c], R["r1_s"].at[g, k, c], R["r1_r"].at[g, k, c],
                         "dp", partner)

        def second(g, k, c):
            return rcopy(s2.at[g, k, c], r2.at[g, k, c], R["r2_s"].at[g, k, c], R["r2_r"].at[g, k, c],
                         "dp", 2 * ahead(g) + core)

        def tell(kind, g):
            d = target(kind, g)
            i = 0 if kind == "mine" else 1
            return rcopy(aux_s.at[d], oaux.at[me], R["ax_s"].at[g, i], R["ax_r"].at[g, i], "dp", d)

        def forward(g, h):
            for k in range(2):
                for c in pieces[h]:
                    first(g, k, c).wait_recv()
                    s2[g, k, c] = (loc[g, k, c].astype(f32) + r1[g, k, c].astype(f32)).astype(bf)
                    second(g, k, c).start()

        def handle(kind, g, h, done, waiting):
            gw = g
            if do_out and g < nx - 1:
                gw = nx - 2 - g
            d = target(kind, gw)
            size = step * piece
            rows = source[d, h * step:(h + 1) * step].reshape(size, feats).astype(f32)
            square = jnp.sum(rows * rows, axis=1, keepdims=True)
            r = lax.broadcasted_iota(jnp.int32, (size, own), 0) + h * size
            c = lax.broadcasted_iota(jnp.int32, (size, own), 1)
            line = jnp.sum(jnp.where(r == c, square, 0.0), axis=0, keepdims=True)
            if h == 0:
                aux_s[d, 0:1, :own] = line
            else:
                aux_s[d, 0:1, :own] += line
            done.append((kind, gw))
            scaled = (rows * R["gain_s"][li:li + 1, :]).astype(bf)
            for k in range(2):
                part = jnp.dot(scaled, weights[k][...], preferred_element_type=f32).astype(bf)
                part = part.reshape(step, piece, wide)
                if kind == "mine":
                    loc[gw, k, h * step:(h + 1) * step] = part
                else:
                    snd[gw, k, h * step:(h + 1) * step] = part
                    for c in pieces[h]:
                        first(gw, k, c).start()
            if done.count((kind, gw)) == halves:
                if (kind, gw) == ("mine", nx - 1):
                    oaux[me] = aux_s[me]
                else:
                    tell(kind, gw).start()
            while waiting:
                forward(*waiting.pop(0))
            if gw < nx - 1:
                pair = [(a, gw, h) for a in ("mine", "other")]
                done.append(("seen", kind, gw, h))
                if all(("seen",) + a in done for a in pair):
                    waiting.append((gw, h))

        def flush(waiting):
            while waiting:
                forward(*waiting.pop(0))

    if do_in:
        bring("gain").wait()
        if not do_out:
            bring("tok").wait()
        for name in ("wb", "wg"):
            load(name, li).wait()
    if not do_out:
        done, waiting = [], []
        for group in groups:
            handle(*group, done, waiting)
        flush(waiting)
    else:
        def finish(i, done, waiting):
            if do_in:
                handle(*groups[i], done, waiting)

        if ntp == 1:
            done, waiting = [], []
            for i in range(len(groups)):
                product_out(i)
                for p in range(i * step, (i + 1) * step):
                    settle(p, psum[p])
                finish(i, done, waiting)
            if do_in:
                flush(waiting)
        else:
            if ntp > 2:
                @pl.when(outer)
                def _():
                    done, waiting = [], []
                    for i in range(len(groups)):
                        product_out(i)
                        for p in range(i * step, (i + 1) * step):
                            if ntp == 4:
                                zsum[p] = psum[p].astype(bf)
                            else:
                                @pl.when(edge)
                                def _():
                                    zsum[p] = psum[p].astype(bf)

                                @pl.when(inner)
                                def _():
                                    zsum[p] = gathered(p).astype(bf)
                            up(p).start()
                    for i in range(len(groups)):
                        for p in range(i * step, (i + 1) * step):
                            down(p).wait_recv()
                            if ntp > 4:
                                @pl.when(inner)
                                def _():
                                    down(p).start()
                            if do_in:
                                flush(waiting)
                        finish(i, done, waiting)
                    if do_in:
                        flush(waiting)
                    for p in range(spots):
                        up(p).wait_send()
                        if ntp > 4:
                            @pl.when(inner)
                            def _():
                                down(p).wait_send()

            @pl.when(center)
            def _():
                done, waiting = [], []
                lag = 4
                for p in range(spots + lag):
                    if p < spots:
                        if p % step == 0:
                            product_out(p // step)
                        zsum[p] = (gathered(p) if ntp > 2 else psum[p]).astype(bf)
                        cross(p).start()
                    if do_in:
                        flush(waiting)
                    q = p - lag
                    if q >= 0:
                        cross(q).wait_recv()
                        settle(q, zsum[q].astype(f32) + zcross[q].astype(f32))
                        if ntp > 2:
                            down(q).start()
                        if q % step == step - 1:
                            finish(q // step, done, waiting)
                if do_in:
                    flush(waiting)
                for p in range(spots):
                    cross(p).wait_send()
                    if ntp > 2:
                        down(p).wait_send()

        for c in range(chunks):
            near(c).wait_send()
            for g in range(nx - 1):
                across(g, c).wait_send()
                passed(g, c).wait_send()

    if do_out and do_in:
        keep = pltpu.make_async_copy(fresh, R["fresh_o"], R["fresh_m"])
        keep.start()
    if do_in:
        last = nx - 1
        for g in range(nx):
            for i, kind in enumerate(("mine", "other")):
                if (kind, g) != ("mine", last):
                    tell(kind, g).wait_recv()
        total = oaux[0, 0:1, :own]
        for d in range(1, ndp):
            total = total + oaux[d, 0:1, :own]
        inv_row = lax.rsqrt(total / (feats * ndp) + epsilon)
        r = lax.broadcasted_iota(jnp.int32, (own, own), 0)
        c = lax.broadcasted_iota(jnp.int32, (own, own), 1)
        inv = jnp.sum(jnp.where(r == c, inv_row, 0.0), axis=1, keepdims=True)
        for h in range(halves):
            for k, out in ((0, ob), (1, og)):
                for c in pieces[h]:
                    first(last, k, c).wait_recv()
                    total = loc[last, k, c].astype(f32) + r1[last, k, c].astype(f32)
                    for g in range(nx - 1):
                        second(g, k, c).wait_recv()
                        total = total + r2[g, k, c].astype(f32)
                    out[c * piece:(c + 1) * piece, :] = (
                        total * inv[c * piece:(c + 1) * piece, :]
                    ).astype(bf)
        if do_out:
            keep.wait()
        for g in range(nx):
            for kind in ("mine", "other"):
                if (kind, g) != ("mine", last):
                    tell(kind, g).wait_send()
            for k in range(2):
                for c in range(chunks):
                    first(g, k, c).wait_send()
                    if g < last:
                        second(g, k, c).wait_send()


def bridge(ndp, ntp, lanes, name, cid, limit, tok, lo=None, li=None, mixed=None, w_out=None, gain=None,
           w_branch=None, w_gate=None):
    f32 = jnp.float32
    bf = jnp.bfloat16
    do_out = mixed is not None
    do_in = w_branch is not None
    nx = ndp // 2
    far = max(nx - 1, 1)
    chunks, piece, feats = tok.shape[1:]
    own = chunks * piece
    spots = ndp * chunks
    weight = pl.BlockSpec(memory_space=pl.ANY)
    sem = pltpu.SemaphoreType.DMA
    names, args, specs, outs, scratch = [], [], [], [], []

    def take(key, a, spec=VM):
        names.append(key)
        args.append(a)
        specs.append(spec)

    take("tok", tok, weight)
    if do_out:
        width = mixed.shape[-1]
        take("m", mixed.reshape(chunks, piece, width), weight)
        take("wo", w_out, weight)
    if do_in:
        width = w_branch.shape[-1]
        take("gain", gain, weight)
        take("wb", w_branch, weight)
        take("wg", w_gate, weight)

    def give(key, shape, dtype):
        names.append(key)
        outs.append(jax.ShapeDtypeStruct(shape, dtype))

    if do_out:
        give("fresh_o" if do_in else "fresh", tok.shape, bf)
    if do_in:
        give("ob", (own, width), bf)
        give("og", (own, width), bf)

    def room(key, shape, dtype):
        names.append(key)
        scratch.append(pltpu.VMEM(shape, dtype))

    def flag(key, *shape):
        names.append(key)
        scratch.append(sem(shape) if shape else sem)

    def sems(key, *shape):
        flag(key + "_s", *shape)
        flag(key + "_r", *shape)

    room("tok_s", tok.shape, bf)
    flag("tok_m")
    if do_in:
        room("gain_s", gain.shape, f32)
        flag("gain_m")
    if do_out:
        room("m_s", (chunks, piece, width), bf)
        flag("m_m")
        if do_in:
            room("fresh", tok.shape, bf)
            flag("fresh_m")
        room("got", (nx, 2, chunks, piece, width), bf)
        room("psum", (spots, piece, feats), f32)
        room("wo_s", w_out.shape[1:], bf)
        flag("wo_m")
        for key in ("zsum", "zin", "zcross"):
            room(key, (spots, piece, feats), bf)
        sems("ga", far, chunks)
        sems("gf", far, chunks)
        sems("gp", chunks)
        for key in ("zi", "zc", "zo"):
            sems(key, spots)
    if do_in:
        for key, a in (("wb", w_branch), ("wg", w_gate)):
            room(key + "_s", a.shape[1:], bf)
            flag(key + "_m")
        room("aux_s", (ndp, 8, lanes), f32)
        room("oaux", (ndp, 8, lanes), f32)
        for key, count in (("snd", nx), ("loc", nx), ("r1", nx), ("s2", far), ("r2", far)):
            room(key, (count, 2, chunks, piece, width), bf)
        sems("r1", nx, 2, chunks)
        sems("r2", far, 2, chunks)
        sems("ax", nx, 2)
    return pl.pallas_call(
        functools.partial(bridge_kernel, ndp, ntp, do_out, do_in, lo, li, names),
        out_shape=tuple(outs),
        in_specs=specs,
        out_specs=((weight, VM, VM) if do_out and do_in else (VM,) * len(outs)),
        scratch_shapes=scratch,
        compiler_params=pltpu.CompilerParams(
            collective_id=cid, has_side_effects=True, vmem_limit_bytes=limit
        ),
        name=name,
    )(*args)


def cell_kernel(layer, heads, steps, cnt_any, cvec_any, br_any, gt_any, mrow_any, bi_any, bf_any, st_any,
                cw_any, wi_any, wf_any, og_any, sg_any, wq_ref, wk_ref, wv_ref, mem_ref, *rest):
    (mixed_any, nc_any, newmem_ref, nmax_any,
     cnt_ref, cvec_ref, br_ref, gt_ref, mrow_ref, bi_ref, bf_ref, st_ref, cw_ref, wi_ref, wf_ref, og_ref,
     sg_ref, mixed_ref, nc_ref, nmax_ref,
     pad_s, conv_s, q_s, k_s, v_s, num_s, car_s, dec_s, cs_s, nc_s, w_s, stage, ins, outs,
     w_sem, s_sem, o_sem) = rest[-37:]
    f32 = jnp.float32
    bf = jnp.bfloat16
    batch = stage.shape[0]
    own, width = br_ref.shape
    dim = HEAD_DIM
    base = 8 - (CONV - 1)

    def fetch(b):
        return pltpu.make_async_copy(mem_ref.at[layer, b], stage.at[b], ins.at[b])

    def store(b):
        return pltpu.make_async_copy(stage.at[b], newmem_ref.at[layer, b], outs.at[b])

    maps = [
        pltpu.make_async_copy(w_ref.at[layer], w_s.at[i], w_sem.at[i])
        for i, w_ref in enumerate((wq_ref, wk_ref, wv_ref))
    ]
    smalls = [
        pltpu.make_async_copy(a, b, s_sem.at[i])
        for i, (a, b) in enumerate((
            (br_any, br_ref), (st_any.at[layer], st_ref), (cw_any, cw_ref), (cnt_any, cnt_ref),
            (cvec_any, cvec_ref), (mrow_any, mrow_ref), (bi_any, bi_ref), (bf_any, bf_ref),
            (wi_any, wi_ref), (wf_any, wf_ref), (og_any, og_ref), (sg_any, sg_ref), (gt_any, gt_ref),
        ))
    ]
    for cp in smalls[:8]:
        cp.start()
    for cp in maps:
        cp.start()
    for cp in smalls[8:]:
        cp.start()

    @pl.loop(0, batch)
    def _(b):
        fetch(b).start()
    for cp in smalls:
        cp.wait()

    r = lax.broadcasted_iota(jnp.int32, (own, own), 0)
    c = lax.broadcasted_iota(jnp.int32, (own, own), 1)
    row = lax.broadcasted_iota(jnp.int32, (own, batch), 0)
    seq = lax.broadcasted_iota(jnp.int32, (own, batch), 1)
    belongs = (row // steps) == seq
    closing = row == seq * steps + (steps - 1)
    nt = (((1,), (1,)), ((), ()))
    spread = jnp.where(belongs, 1.0, 0.0)
    counts = jnp.broadcast_to(cvec_ref[...].astype(f32), (8, batch))
    count_row = lax.dot_general(counts, spread, nt, preferred_element_type=f32)[0:1, :]
    count_col = jnp.sum(jnp.where(belongs, counts[0:1, :], 0.0), axis=1, keepdims=True)
    branch = br_ref[...]
    pad_s[:, 8:8 + steps, :] = branch.astype(f32).reshape(batch, steps, width)
    for j in range(CONV - 1):
        rows = st_ref[j].astype(f32)
        for b in range(batch):
            pad_s[b, base + j:base + j + 1, :] = rows[b:b + 1, :]
    total = pad_s[:, base:base + steps, :] * cw_ref[layer, 0:1, :]
    for j in range(1, CONV):
        total = total + pad_s[:, base + j:base + j + steps, :] * cw_ref[layer, j:j + 1, :]
    conv = (total * jax.nn.sigmoid(total)).astype(bf).reshape(own, width)
    conv_s[...] = conv
    for b in range(batch):
        for i in range(CONV - 1):
            nc_s[i, b:b + 1, :] = pad_s[b, pl.ds(base + i + cnt_ref[b], 1), :]
    nc_ref[...] = nc_s[...].astype(bf)

    same = (r // steps) == (c // steps)
    causal = same & (r >= c)
    behind = same & (r <= c)
    live_col = (r[:, 0:1] % steps).astype(f32) < count_col
    live_row = (c[0:1, :] % steps).astype(f32) < count_row
    for cp in maps:
        cp.wait()
    def log_sig(x):
        return jnp.minimum(x, 0.0) - jnp.log1p(jnp.exp(-jnp.abs(x)))

    def side(columns):
        lane = lax.broadcasted_iota(jnp.int32, (own, heads), 1)
        out = jnp.broadcast_to(columns[0], (own, heads))
        for h in range(1, heads):
            out = jnp.where(lane == h, columns[h], out)
        return out

    def pile(lines):
        level = lax.broadcasted_iota(jnp.int32, (heads, own), 0)
        out = jnp.broadcast_to(lines[0], (heads, own))
        for h in range(1, heads):
            out = jnp.where(level == h, lines[h], out)
        return out

    exact = lax.Precision.HIGHEST
    cols = ([], [])
    lines = ([], [])
    for h in range(heads):
        sl = slice(h * dim, (h + 1) * dim)
        q = jnp.dot(conv[:, sl], w_s[0, h], preferred_element_type=f32).astype(bf)
        k = jnp.dot(conv[:, sl], w_s[1, h], preferred_element_type=f32).astype(bf)
        v = jnp.dot(branch[:, sl], w_s[2, h], preferred_element_type=f32).astype(bf)
        q_s[:, sl] = q.astype(f32)
        k_s[:, sl] = k.astype(f32) * (dim ** -0.5)
        v_s[:, sl] = v.astype(f32)
        for n, g_ref in enumerate((wi_ref, wf_ref)):
            col = None
            for i, part in enumerate((q, k, v)):
                w = g_ref[layer, :, i * dim:(i + 1) * dim]
                if heads == 1:
                    w = jnp.broadcast_to(w.astype(f32), (8, dim)).astype(bf)
                one = lax.dot_general(part, w, nt, preferred_element_type=f32)
                two = lax.dot_general(w, part, nt, preferred_element_type=f32)
                col, line = (one, two) if col is None else (col + one, line + two)
            cols[n].append(col[:, h:h + 1])
            lines[n].append(line[h:h + 1, :])
    bias_col = [ref[layer:layer + 1, :] for ref in (bi_ref, bf_ref)]
    head_eye = (
        lax.broadcasted_iota(jnp.int32, (heads, heads), 0) == lax.broadcasted_iota(jnp.int32, (heads, heads), 1)
    )
    bias_row = [jnp.sum(jnp.where(head_eye, b, 0.0), axis=1, keepdims=True) for b in bias_col]
    ig_col = jnp.where(live_col, side(cols[0]) + bias_col[0], very_negative)
    fg_col = jnp.where(live_col, log_sig(side(cols[1]) + bias_col[1]), 0.0)
    ig_row = jnp.where(live_row, pile(lines[0]) + bias_row[0], very_negative)
    fg_row = jnp.where(live_row, log_sig(pile(lines[1]) + bias_row[1]), 0.0)
    ones = jnp.where(causal, 1.0, 0.0)
    sames = jnp.where(same, 1.0, 0.0)
    if heads == 1:
        cum_col = jnp.sum(jnp.where(causal, fg_row, 0.0), axis=1, keepdims=True)
        end_col = jnp.sum(jnp.where(same, fg_row, 0.0), axis=1, keepdims=True)
        cum_row = jnp.sum(jnp.where(behind, fg_col, 0.0), axis=0, keepdims=True)
        old_max = jnp.sum(jnp.where(belongs, mrow_ref[layer], 0.0), axis=1, keepdims=True)
    else:
        cum_col = jnp.dot(ones, fg_col, preferred_element_type=f32, precision=exact)
        end_col = jnp.dot(sames, fg_col, preferred_element_type=f32, precision=exact)
        cum_row = lax.dot_general(fg_row, ones, nt, preferred_element_type=f32, precision=exact)
        old_max = lax.dot_general(spread, mrow_ref[layer], nt, preferred_element_type=f32, precision=exact)
    lift_row = ig_row - cum_row
    carried = cum_col + old_max
    tops = []
    ends_ = []
    for h in range(heads):
        lift = lift_row[h:h + 1, :]
        logw = jnp.where(causal, cum_col[:, h:h + 1] + lift, very_negative)
        tops.append(jnp.max(logw, axis=1, keepdims=True))
        ends_.append(jnp.max(jnp.where(same, lift, very_negative), axis=1, keepdims=True))
    stab = jnp.maximum(side(tops), carried)
    new_max = jnp.maximum(end_col + side(ends_), end_col + old_max)
    update = jnp.exp(end_col - cum_col + ig_col - new_max)
    dec_s[:, :heads] = jnp.exp(end_col + old_max - new_max)
    cs_s[:, :heads] = jnp.exp(carried - stab)
    for h in range(heads):
        sl = slice(h * dim, (h + 1) * dim)
        logw = jnp.where(causal, cum_col[:, h:h + 1] + lift_row[h:h + 1, :], very_negative)
        weights = jnp.exp(logw - stab[:, h:h + 1])
        nmax_ref[h:h + 1, :] = jnp.sum(jnp.where(closing, new_max[:, h:h + 1], 0.0), axis=0, keepdims=True)
        scores = lax.dot_general(q_s[:, sl].astype(bf), k_s[:, sl].astype(bf), nt, preferred_element_type=f32)
        scores = (jnp.where(causal, scores, 0.0) * weights).astype(bf)
        num_s[:, sl] = jnp.dot(scores, v_s[:, sl].astype(bf), preferred_element_type=f32)
        k_s[:, sl] = k_s[:, sl] * update[:, h:h + 1]

    def advance(b):
        fetch(b).wait()
        rows = pl.ds(pl.multiple_of(b * steps, 8), steps)
        for h in range(heads):
            sl = slice(h * dim, (h + 1) * dim)
            old = stage[b, h]
            car_s[rows, sl] = jnp.dot(q_s[rows, sl].astype(bf), old.astype(bf), preferred_element_type=f32)
            outer = lax.dot_general(
                k_s[rows, sl].astype(bf), v_s[rows, sl].astype(bf), (((0,), (0,)), ((), ())),
                preferred_element_type=f32,
            )
            stage[b, h] = dec_s[rows, :][0:1, h:h + 1] * old + outer
        store(b).start()

    stride = 2 if batch % 2 == 0 else 1

    @pl.loop(0, batch, step=stride)
    def _(b):
        for i in range(stride):
            advance(b + i)

    counts = jnp.broadcast_to(cvec_ref[...].astype(f32), (8, batch))
    row = lax.broadcasted_iota(jnp.int32, (own, batch), 0)
    seq = lax.broadcasted_iota(jnp.int32, (own, batch), 1)
    count_col = jnp.sum(jnp.where((row // steps) == seq, counts[0:1, :], 0.0), axis=1, keepdims=True)
    live = (lax.broadcasted_iota(jnp.int32, (own, 1), 0) % steps).astype(f32) < count_col
    for h in range(heads):
        sl = slice(h * dim, (h + 1) * dim)
        num = num_s[:, sl] + cs_s[:, h:h + 1] * car_s[:, sl]
        centered = num - jnp.mean(num, axis=1, keepdims=True)
        normal = centered * lax.rsqrt(jnp.mean(centered * centered, axis=1, keepdims=True) + epsilon)
        gate = gt_ref[:, sl].astype(f32)
        mixed = normal * og_ref[layer, h:h + 1, :] + sg_ref[layer:layer + 1, sl] * conv_s[:, sl].astype(f32)
        mixed = mixed * (gate * jax.nn.sigmoid(gate))
        mixed_ref[:, sl] = jnp.where(live, mixed, 0.0).astype(bf)
    ends = [
        pltpu.make_async_copy(a, b, o_sem.at[i])
        for i, (a, b) in enumerate((
            (mixed_ref, mixed_any), (nc_ref, nc_any.at[layer]), (nmax_ref, nmax_any.at[layer])
        ))
    ]
    for cp in ends:
        cp.start()
    for b in range(batch):
        store(b).wait()
    for cp in ends:
        cp.wait()


def memory_cell(layer, steps, counts, bias_input, bias_forget, branch, gate, old_max, state, conv_weight,
                w_input_gate, w_forget_gate, out_gain, skip_gain, w_query, w_key, w_value, memory, previous):
    layers, batch, heads, dim, _ = memory.shape
    own, width = branch.shape
    f32 = jnp.float32
    bf = jnp.bfloat16
    anyspace = pl.BlockSpec(memory_space=pl.ANY)
    args = [counts, counts[None, :], branch, gate, old_max, bias_input, bias_forget, state, conv_weight,
            w_input_gate, w_forget_gate, out_gain, skip_gain, w_query, w_key, w_value, memory]
    held = [pltpu.SMEM(counts.shape, jnp.int32)]
    held += [pltpu.VMEM(a.shape[1:] if a is state else a.shape, a.dtype) for a in args[1:13]]
    held += [
        pltpu.VMEM((own, width), bf),
        pltpu.VMEM((CONV - 1, batch, width), bf),
        pltpu.VMEM((heads, batch), f32),
    ]
    aliases = {}
    if previous is not None:
        aliases = {len(args): 2, len(args) + 1: 1, len(args) + 2: 3}
        args += list(previous)
    specs = [anyspace] * len(args)
    big = pltpu.VMEM((own, width), f32)
    small = pltpu.VMEM((own, 128), f32)
    return pl.pallas_call(
        functools.partial(cell_kernel, layer, heads, steps),
        out_shape=(
            jax.ShapeDtypeStruct((own, width), jnp.bfloat16),
            jax.ShapeDtypeStruct((layers, CONV - 1, batch, width), jnp.bfloat16),
            jax.ShapeDtypeStruct(memory.shape, f32),
            jax.ShapeDtypeStruct((layers, heads, batch), f32),
        ),
        in_specs=specs,
        out_specs=(anyspace,) * 4,
        scratch_shapes=held + [
            pltpu.VMEM((batch, 8 + steps, width), f32),
            pltpu.VMEM((own, width), jnp.bfloat16),
            big, big, big, big, big, small, small,
            pltpu.VMEM((CONV - 1, batch, width), f32),
            pltpu.VMEM((3, heads, dim, dim), jnp.bfloat16),
            pltpu.VMEM((batch, heads, dim, dim), f32),
            pltpu.SemaphoreType.DMA((batch,)), pltpu.SemaphoreType.DMA((batch,)),
            pltpu.SemaphoreType.DMA((3,)), pltpu.SemaphoreType.DMA((13,)), pltpu.SemaphoreType.DMA((3,)),
        ],
        input_output_aliases=aliases,
        compiler_params=pltpu.CompilerParams(vmem_limit_bytes=FULL_VMEM),
        name="memory_cell",
    )(*args)


def per_device(tokens, live_counts, norm_gain, w_branch, w_silu_gate, conv_weight, w_query, w_key,
               w_value, w_input_gate, w_forget_gate, bias_input, bias_forget, out_gain, skip_gain,
               w_out, conv_state, memory, max_state):
    ndp = lax.axis_size("dp")
    ntp = lax.axis_size("tp")
    steps, features = tokens.shape[1:]
    own = live_counts.shape[0] * steps
    lanes = -(-own // 128) * 128
    chunks = 4 if own % 64 == 0 else 1
    stream = tokens.reshape(ndp, chunks, own // chunks, features)
    old_max = jnp.transpose(max_state, (0, 2, 1))
    states = jnp.transpose(conv_state, (0, 2, 1, 3))
    link = functools.partial(bridge, ndp, ntp, lanes)
    inputs = dict(gain=norm_gain, w_branch=w_branch, w_gate=w_silu_gate)

    branch, gate = link("enter", 0, FULL_VMEM, stream, li=0, **inputs)
    previous = None
    for l in range(LAYERS):
        mixed, new_conv, new_memory, new_max = memory_cell(
            l, steps, live_counts, bias_input, bias_forget, branch, gate, old_max, states, conv_weight,
            w_input_gate, w_forget_gate, out_gain, skip_gain, w_query, w_key, w_value, memory, previous
        )
        previous = (new_memory, new_conv, new_max)
        if l + 1 < LAYERS:
            stream, branch, gate = link(
                f"bridge{l}", l + 1, FULL_VMEM, stream, lo=l, li=l + 1, mixed=mixed, w_out=w_out, **inputs
            )
        else:
            (stream,) = link("leave", l + 1, LEAVE_VMEM, stream, lo=l, mixed=mixed, w_out=w_out)
    return (stream.reshape(tokens.shape), jnp.transpose(new_conv, (0, 2, 1, 3)), new_memory,
            jnp.transpose(new_max, (0, 2, 1)))


def solution(mesh):
    in_specs = (
        P("grp", None, "dp"),
        P(("grp", "dp")),
        P(None, "dp"),
        P(None, "dp", "tp"),
        P(None, "dp", "tp"),
        P(None, None, "tp"),
        P(None, "tp", None, None),
        P(None, "tp", None, None),
        P(None, "tp", None, None),
        P(None, "tp", None),
        P(None, "tp", None),
        P(None, "tp"),
        P(None, "tp"),
        P(None, "tp", None),
        P(None, "tp"),
        P(None, "tp", "dp"),
        P(None, ("grp", "dp"), None, "tp"),
        P(None, ("grp", "dp"), "tp", None, None),
        P(None, ("grp", "dp"), "tp"),
    )
    out_specs = (
        P("grp", None, "dp"),
        P(None, ("grp", "dp"), None, "tp"),
        P(None, ("grp", "dp"), "tp", None, None),
        P(None, ("grp", "dp"), "tp"),
    )
    return jax.shard_map(
        per_device, mesh=mesh, in_specs=in_specs, out_specs=out_specs, check_vma=False
    )
```
